32 devices in a mesh: sp: 8 (over z, y), tp: 4 (over x, core).
Axes of the slice: x: 2, y: 2, z: 4, core: 2. Of those that a mesh axis runs over, the one named last changes fastest.
Arguments:
- residual: bfloat16 [3072, 2048], P(('sp', 'tp')), may hold values from -6 to 6
- query_one: bfloat16 [3072, 512], P('sp', 'tp'), may hold values from -6 to 6
- key_one: bfloat16 [3072, 512], P('sp', 'tp'), may hold values from -6 to 6
- value_one: bfloat16 [3072, 1024], P('sp', 'tp'), may hold values from -6 to 6
- gate_one: bfloat16 [3072, 1024], P('sp', 'tp'), may hold values from -6 to 6
- decay_one: bfloat16 [2, 3072, 512], P(None, 'sp', 'tp'), may hold values from -12 to 12
- norm_one: float32 [128], replicated, may hold values from 0.1 to 1.9
- output_one: bfloat16 [1024, 2048], P('tp'), may hold values from -0.125 to 0.125
- query_two: bfloat16 [3072, 1024], P('sp', 'tp'), may hold values from -6 to 6
- key_two: bfloat16 [3072, 1024], P('sp', 'tp'), may hold values from -6 to 6
- value_two: bfloat16 [3072, 1024], P('sp', 'tp'), may hold values from -6 to 6
- gate_two: bfloat16 [3072, 1024], P('sp', 'tp'), may hold values from -6 to 6
- decay_two: bfloat16 [2, 3072, 1024], P(None, 'sp', 'tp'), may hold values from -12 to 12
- norm_two: float32 [128], replicated, may hold values from 0.1 to 1.9
- output_two: bfloat16 [1024, 2048], P('tp'), may hold values from -0.125 to 0.125
- norm_gain: float32 [2048], replicated, may hold values from 0.1 to 1.9
- expert_ids: int32 [3072, 2], P('sp'), may hold values from 0 to 7, as said below
- group_weight: float32 [3072], P('sp'), may hold values from 0.25 to 1
- pair_weight: float32 [3072, 2], P('sp'), may hold values from 0.05 to 1
- expert_gate: bfloat16 [8, 2048, 1024], P('sp', None, 'tp'), may hold values from -0.125 to 0.125
- expert_up: bfloat16 [8, 2048, 1024], P('sp', None, 'tp'), may hold values from -0.125 to 0.125
- expert_down: bfloat16 [8, 1024, 2048], P('sp', 'tp'), may hold values from -0.1875 to 0.1875
Outputs:
- layer_out: bfloat16 [3072, 2048], P(('sp', 'tp'))
The draws below stay inside these ranges and needn't reach their ends.
Inputs may be any that keep to these rules, and one draw needn't show every extreme that they name: `expert_ids`: each row names two different experts of one group, the group of expert e being e // 2. In each aligned block of 96 rows no expert is named more than 49 times, and one expert, the same in every block, is named exactly 49 times in each block.
All inputs are finite; a program needn't handle non-finite values.
Results may differ from the reference program's by a relative error of at most 0.018.
Values may be sent and summed in bfloat16 or wider, within the bound.
A program may use at most 128 MiB of HBM per device.

```python
import math
from functools import partial
import jax
import jax.numpy as jnp
from jax import lax

D = 2048
HEADS_ONE = 8
KEY_ONE = 64
HEADS_TWO = 8
KEY_TWO = 128
VALUE_W = 128
FF = 1024
BLOCK = 64
GROUPS = 4
TOK_DEV = 384
SEQUENCE_TOKENS = 3072
ROWS_DEV = 96
EXPERTS = 8
EXP_GROUP = 2
CAPACITY = 49
N_TP = 4


def decay_law(key, channels):
    random_keys = jax.random.split(key, 6)
    slow = jax.random.uniform(random_keys[0], (2, 1, channels)) < 0.5
    random_jitter = 0.5 * jax.random.normal(random_keys[1], (2, SEQUENCE_TOKENS, channels))
    channel_factor = jnp.exp(jax.random.uniform(random_keys[2], (2, 1, channels), minval=math.log(0.5), maxval=math.log(1.5)))
    device_factor = jnp.exp(jax.random.uniform(random_keys[3], (2, SEQUENCE_TOKENS // TOK_DEV, 1), minval=math.log(0.5), maxval=math.log(1.5)))
    device_factor = jnp.repeat(device_factor, TOK_DEV, axis=1)
    slow_rate = 0.35 * channel_factor * device_factor / SEQUENCE_TOKENS
    fast_rate = 1.0 / (BLOCK * channel_factor)
    rate = jnp.where(slow, slow_rate, fast_rate)
    smoothed_values = -jnp.log(jnp.expm1(16.0 * rate)) + random_jitter
    spike_position = jax.random.randint(random_keys[4], (2, 2, 1), 0, SEQUENCE_TOKENS)
    retained_entries = jax.random.uniform(random_keys[5], (2, 2, 1), minval=0.5, maxval=0.8)
    spike_value = -jnp.log(jnp.expm1(-16.0 * jnp.log(retained_entries)))
    token_positions = jnp.arange(SEQUENCE_TOKENS, dtype=jnp.int32)[None, None, :]
    match_flags = token_positions == spike_position
    spike_row = jnp.sum(jnp.where(match_flags, spike_value, 0.0), axis=1)
    any_match_found = jnp.any(match_flags, axis=1)
    final_output = jnp.where(any_match_found[:, :, None], spike_row[:, :, None] + 0.1 * random_jitter, smoothed_values)
    return jnp.clip(final_output, -12.0, 12.0).astype(jnp.bfloat16)


def draw_decay_one(key, part):
    return decay_law(jax.random.fold_in(key, 11), HEADS_ONE * KEY_ONE)


def draw_decay_two(key, part):
    return decay_law(jax.random.fold_in(key, 12), HEADS_TWO * KEY_TWO)


def route_block(key, hot):
    order_key, group_key, member_key = jax.random.split(key, 3)
    order = jax.random.permutation(order_key, ROWS_DEV).astype(jnp.int32)
    group_score = jax.random.randint(group_key, (ROWS_DEV, GROUPS), 0, 1 << 20) * GROUPS + jnp.arange(GROUPS, dtype=jnp.int32)
    member_score = jax.random.randint(member_key, (ROWS_DEV, EXPERTS), 0, 1 << 20) * EXPERTS + jnp.arange(EXPERTS, dtype=jnp.int32)
    labels = jnp.arange(EXPERTS, dtype=jnp.int32)

    def place_row(counts, step):
        row = order[step]
        forced = step < CAPACITY
        free = counts < CAPACITY
        usable = jnp.sum(free.reshape(GROUPS, EXP_GROUP).astype(jnp.int32), axis=1) >= 2
        picked_group = jnp.argmax(jnp.where(usable, group_score[row], -1)).astype(jnp.int32)
        chosen_group = jnp.where(forced, hot // EXP_GROUP, picked_group)
        allowed = free & (labels // EXP_GROUP == chosen_group)
        scored = jnp.where(allowed, member_score[row], -1)
        first = jnp.where(forced, hot, jnp.argmax(scored).astype(jnp.int32))
        second = jnp.argmax(jnp.where(labels == first, -1, scored)).astype(jnp.int32)
        counts = counts + (labels == first).astype(jnp.int32) + (labels == second).astype(jnp.int32)
        return (counts, (row, first, second))
    _, (rows, firsts, seconds) = lax.scan(place_row, jnp.zeros((EXPERTS,), jnp.int32), jnp.arange(ROWS_DEV, dtype=jnp.int32))
    return jnp.zeros((ROWS_DEV, 2), jnp.int32).at[rows].set(jnp.stack([firsts, seconds], axis=1))


def draw_expert_ids(key, part):
    hot_key, block_key = jax.random.split(jax.random.fold_in(key, 21))
    hot = jax.random.randint(hot_key, (), 0, EXPERTS).astype(jnp.int32)
    random_keys = jax.random.split(block_key, SEQUENCE_TOKENS // ROWS_DEV)
    blocks = jax.vmap(partial(route_block, hot=hot))(random_keys)
    return blocks.reshape(SEQUENCE_TOKENS, 2)


def levels(key, shape, shards, low, high):
    level = 1.0
    for axis_at, shards_of in shards:
        draws = jax.random.uniform(jax.random.fold_in(jax.random.fold_in(key, 6), axis_at), (shards_of,), jnp.float32, low / len(shards), high / len(shards))
        level = level * jnp.repeat(jnp.exp(draws), shape[axis_at] // shards_of).reshape((-1,) + (1,) * (len(shape) - 1 - axis_at))
    return level


def bell_draw(rng, shape, spread, most, shards=(), kind=jnp.bfloat16):
    values = spread * jax.random.normal(rng, shape, jnp.float32)
    if shards:
        values = values * levels(rng, shape, shards, -0.22, 0.18)
    return jnp.clip(values, -most, most).astype(kind)


def setup_inputs(seed: int = 0) -> dict:
    streams_of = jax.random.split(jax.random.key(seed), 23)
    return {
        "residual": bell_draw(streams_of[0], (SEQUENCE_TOKENS, D), 1.0, 6.0, ((0, 32),)),
        "query_one": bell_draw(streams_of[1], (SEQUENCE_TOKENS, HEADS_ONE * KEY_ONE), 1.0, 6.0, ((0, 8), (1, 4))),
        "key_one": bell_draw(streams_of[2], (SEQUENCE_TOKENS, HEADS_ONE * KEY_ONE), 1.0, 6.0, ((0, 8), (1, 4))),
        "value_one": bell_draw(streams_of[3], (SEQUENCE_TOKENS, HEADS_ONE * VALUE_W), 1.0, 6.0, ((0, 8), (1, 4))),
        "gate_one": bell_draw(streams_of[4], (SEQUENCE_TOKENS, HEADS_ONE * VALUE_W), 1.0, 6.0, ((0, 8), (1, 4))),
        "decay_one": draw_decay_one(jax.random.fold_in(streams_of[22], 71), 0),
        "norm_one": jnp.clip(1.0 + 0.18 * jax.random.normal(streams_of[6], (VALUE_W,), jnp.float32), 0.1, 1.9),
        "output_one": bell_draw(streams_of[7], (HEADS_ONE * VALUE_W, D), ((HEADS_ONE + HEADS_TWO) * VALUE_W) ** -0.5, 0.125, ((0, 4),)),
        "query_two": bell_draw(streams_of[8], (SEQUENCE_TOKENS, HEADS_TWO * KEY_TWO), 1.0, 6.0, ((0, 8), (1, 4))),
        "key_two": bell_draw(streams_of[9], (SEQUENCE_TOKENS, HEADS_TWO * KEY_TWO), 1.0, 6.0, ((0, 8), (1, 4))),
        "value_two": bell_draw(streams_of[10], (SEQUENCE_TOKENS, HEADS_TWO * VALUE_W), 1.0, 6.0, ((0, 8), (1, 4))),
        "gate_two": bell_draw(streams_of[11], (SEQUENCE_TOKENS, HEADS_TWO * VALUE_W), 1.0, 6.0, ((0, 8), (1, 4))),
        "decay_two": draw_decay_two(jax.random.fold_in(streams_of[22], 71), 0),
        "norm_two": jnp.clip(1.0 + 0.18 * jax.random.normal(streams_of[13], (VALUE_W,), jnp.float32), 0.1, 1.9),
        "output_two": bell_draw(streams_of[14], (HEADS_TWO * VALUE_W, D), ((HEADS_ONE + HEADS_TWO) * VALUE_W) ** -0.5, 0.125, ((0, 4),)),
        "norm_gain": jnp.clip(1.0 + 0.18 * jax.random.normal(streams_of[15], (D,), jnp.float32), 0.1, 1.9),
        "expert_ids": draw_expert_ids(jax.random.fold_in(streams_of[22], 71), 0),
        "group_weight": jnp.clip(jnp.exp(math.log(1.0) - 1.3862944 * jax.random.uniform(streams_of[17], (SEQUENCE_TOKENS,), jnp.float32) ** levels(streams_of[17], (SEQUENCE_TOKENS,), ((0, 8),), -0.2, 0.2)), 0.25, 1.0),
        "pair_weight": jnp.clip(jnp.exp(math.log(1.0) - 2.9957323 * jax.random.uniform(streams_of[18], (SEQUENCE_TOKENS, 2), jnp.float32) ** levels(streams_of[18], (SEQUENCE_TOKENS, 2), ((0, 8),), -0.2, 0.2)), 0.05, 1.0),
        "expert_gate": bell_draw(streams_of[19], (EXPERTS, D, FF), D ** -0.5, 0.125, ((0, 8), (2, 4))),
        "expert_up": bell_draw(streams_of[20], (EXPERTS, D, FF), D ** -0.5, 0.125, ((0, 8), (2, 4))),
        "expert_down": bell_draw(streams_of[21], (EXPERTS, FF, D), FF ** -0.5, 0.1875, ((0, 8), (1, 4))),
    }


HIGH = lax.Precision.HIGHEST
TAU = 16.0
EPS = 1e-06

def advance(state_now, step_input):
    fade_rate, extra_term = step_input
    return (fade_rate[..., None] * state_now + extra_term, state_now)

def block_pass(queries, key_rows, values, rates):
    length, heads, width = queries.shape
    blocks = length // BLOCK
    shaped = (blocks, BLOCK, heads, width)
    cumul = jnp.cumsum(rates.reshape(shaped), axis=1)
    block_end = cumul[:, -1]
    key_blocks = key_rows.reshape(shaped)
    value_blocks = values.reshape(blocks, BLOCK, heads, values.shape[-1])
    query_dec = queries.reshape(shaped) * jnp.exp(cumul)
    query_low = query_dec.astype(jnp.bfloat16)
    key_dec = (key_blocks * jnp.exp(-cumul)).astype(jnp.bfloat16)
    key_end = (key_blocks * jnp.exp(block_end[:, None] - cumul)).astype(jnp.bfloat16)
    lower_mask = jnp.tril(jnp.ones((BLOCK, BLOCK), jnp.float32))
    scores = jnp.einsum('nthd,nshd->nhts', query_low, key_dec, preferred_element_type=jnp.float32) * lower_mask
    scores = scores.astype(jnp.bfloat16)
    inner_part = jnp.einsum('nhts,nshe->nthe', scores, value_blocks, preferred_element_type=jnp.float32)
    added = jnp.einsum('nshd,nshe->nhde', key_end, value_blocks, preferred_element_type=jnp.float32)
    empty = jnp.zeros((heads, width, values.shape[-1]), jnp.float32)
    state_out, before = lax.scan(advance, empty, (jnp.exp(block_end), added))
    outer_part = jnp.einsum('nthd,nhde->nthe', query_dec, before, precision=HIGH)
    return (inner_part + outer_part).reshape(length, heads, values.shape[-1])

def group_mix(query, key_in, value, gate, decay, gain, width):
    heads = query.shape[1] // width
    queries = query.astype(jnp.float32).reshape(SEQUENCE_TOKENS, heads, width) * width ** (-0.5)
    key_rows = key_in.astype(jnp.float32).reshape(SEQUENCE_TOKENS, heads, width)
    values = value.reshape(SEQUENCE_TOKENS, heads, VALUE_W)
    rates = jax.nn.log_sigmoid(decay.astype(jnp.float32)) / TAU
    ahead = block_pass(queries, key_rows, values, rates[0].reshape(SEQUENCE_TOKENS, heads, width))
    behind = block_pass(jnp.flip(queries, 0), jnp.flip(key_rows, 0), jnp.flip(values, 0), jnp.flip(rates[1], 0).reshape(SEQUENCE_TOKENS, heads, width))
    total = ahead + jnp.flip(behind, 0)
    scale = lax.rsqrt(lax.optimization_barrier(jnp.mean(total * total, axis=-1, keepdims=True)) + EPS)
    normed = (total * scale * gain).reshape(SEQUENCE_TOKENS, heads * VALUE_W)
    return (normed * jax.nn.silu(gate.astype(jnp.float32))).astype(jnp.bfloat16)

def rounded(term):
    return lax.optimization_barrier(term.astype(jnp.bfloat16)).astype(jnp.float32)

def slot_table(routes, capacity, experts):
    flat = routes.reshape(-1)
    count = flat.shape[0]
    onehot = (flat[:, None] == jnp.arange(experts, dtype=jnp.int32)[None, :]).astype(jnp.int32)
    place = lax.optimization_barrier(jnp.sum((jnp.cumsum(onehot, axis=0) - onehot) * onehot, axis=1)).astype(jnp.int32)
    table = jnp.full((experts, capacity), count, jnp.int32).at[flat, place].set(jnp.arange(count, dtype=jnp.int32))
    return (table, place)

def reference(residual, query_one, key_one, value_one, gate_one, decay_one, norm_one, output_one, query_two, key_two, value_two, gate_two, decay_two, norm_two, output_two, norm_gain, expert_ids, group_weight, pair_weight, expert_gate, expert_up, expert_down):
    mixed_one = group_mix(query_one, key_one, value_one, gate_one, decay_one, norm_one, KEY_ONE)
    mixed_two = group_mix(query_two, key_two, value_two, gate_two, decay_two, norm_two, KEY_TWO)
    span_one = mixed_one.shape[1] // N_TP
    span_two = mixed_two.shape[1] // N_TP
    projected = jnp.zeros((SEQUENCE_TOKENS, D), jnp.float32)
    for part in range(N_TP):
        term = jnp.dot(mixed_one[:, part * span_one:(part + 1) * span_one], output_one[part * span_one:(part + 1) * span_one], preferred_element_type=jnp.float32)
        term = term + jnp.dot(mixed_two[:, part * span_two:(part + 1) * span_two], output_two[part * span_two:(part + 1) * span_two], preferred_element_type=jnp.float32)
        projected = projected + rounded(term)
    stream = (residual.astype(jnp.float32) + rounded(projected)).astype(jnp.bfloat16)
    wide = stream.astype(jnp.float32)
    normed = (wide * lax.rsqrt(lax.optimization_barrier(jnp.mean(wide * wide, axis=-1, keepdims=True)) + EPS) * norm_gain).astype(jnp.bfloat16)
    weights = group_weight[:, None] * pair_weight / lax.optimization_barrier(jnp.sum(pair_weight, axis=1, keepdims=True))
    blocks = SEQUENCE_TOKENS // ROWS_DEV
    tables, places = jax.vmap(partial(slot_table, capacity=CAPACITY, experts=EXPERTS))(expert_ids.reshape(blocks, ROWS_DEV, 2))
    offsets = (jnp.arange(blocks, dtype=jnp.int32) * (2 * ROWS_DEV))[:, None, None]
    assigned = jnp.where(tables == 2 * ROWS_DEV, 2 * SEQUENCE_TOKENS, tables + offsets).astype(jnp.int32)
    assigned = jnp.transpose(assigned, (1, 0, 2)).reshape(EXPERTS, blocks * CAPACITY)
    padded = jnp.concatenate([normed, jnp.zeros((1, D), jnp.bfloat16)], axis=0)
    route_weight = jnp.concatenate([weights.reshape(-1), jnp.zeros((1,), jnp.float32)])
    span = FF // N_TP

    def expert_pass(total, step_input):
        index, weight_gate, weight_up, weight_down = step_input
        token = index // 2
        rows = padded[token]
        gate_part = jnp.dot(rows, weight_gate, preferred_element_type=jnp.float32)
        up_part = jnp.dot(rows, weight_up, preferred_element_type=jnp.float32)
        hidden = (jax.nn.silu(gate_part) * up_part).astype(jnp.bfloat16)
        summed = jnp.zeros((rows.shape[0], D), jnp.float32)
        for part in range(N_TP):
            summed = summed + rounded(jnp.dot(hidden[:, part * span:(part + 1) * span], weight_down[part * span:(part + 1) * span], preferred_element_type=jnp.float32))
        final_output = rounded(summed)
        return (total.at[token].add(route_weight[index][:, None] * final_output), None)
    total, _ = lax.scan(expert_pass, jnp.zeros((SEQUENCE_TOKENS + 1, D), jnp.float32), (assigned, expert_gate, expert_up, expert_down))
    return (stream.astype(jnp.float32) + total[:SEQUENCE_TOKENS]).astype(jnp.bfloat16)
```

```python
import functools

import jax
import jax.numpy as jnp
from jax import lax
from jax.experimental import pallas as pl
from jax.experimental.pallas import tpu as pltpu
from jax.sharding import PartitionSpec as P

D = 2048
KEY_ONE = 64
KEY_TWO = 128
VALUE_W = 128
BLOCK = 64
GROUPS = 4


MESH = pl.DeviceIdType.MESH
TAU = 16.0
EPS = 1e-06


def log_sigmoid(x):
    return jnp.minimum(x, 0.0) - jnp.log1p(jnp.exp(-jnp.abs(x)))


def contract(a, b, dims):
    return lax.dot_general(a, b, (dims, ((), ())), preferred_element_type=jnp.float32)


NN, NT, TN = ((1,), (0,)), ((1,), (1,)), ((0,), (0,))


def flip_bit(index, bit):
    return index + bit - 2 * bit * lax.rem(index // bit, 2)


def meet(peers):
    barrier = pltpu.get_barrier_semaphore()
    for peer in peers:
        pl.semaphore_signal(barrier, inc=1, device_id=peer, device_id_type=MESH)
    pl.semaphore_wait(barrier, len(peers))


def remote(source, target, send, recv, device):
    return pltpu.make_async_remote_copy(
        src_ref=source,
        dst_ref=target,
        send_sem=send,
        recv_sem=recv,
        device_id=device,
        device_id_type=MESH,
    )


def nothing(*_):
    return None


PACK = VALUE_W + 16


def mix(n_sp, n_tp, operands, scratch, ready, sent_states, got_states):
    q1, k1, v1, g1, d1, q2, k2, v2, g2, d2, norm1, norm2, out1, out2, res, gain = operands
    cum, qd, kd, added, ends, sent, got, carried, total, mixed, part_send, part_got = scratch[:12]
    st_send, st_recv, pt_send, pt_recv = scratch[12:]
    sp, tp = lax.axis_index("sp"), lax.axis_index("tp")
    length = q1.shape[0]
    blocks = length // BLOCK
    lanes = 128
    units = []
    for q, k, v, g, d, norm, key in (
        (q1, k1, v1, g1, d1, norm1, KEY_ONE),
        (q2, k2, v2, g2, d2, norm2, KEY_TWO),
    ):
        per = lanes // key
        for at in range(q.shape[1] // lanes):
            units.append((q, k, v, g, d, norm, key, per, at))
    count = len(units)
    bits = [1 << r for r in range(n_tp.bit_length() - 1)]

    meet(
        [(lax.rem(sp + off, n_sp), tp) for off in range(1, n_sp)]
        + [(sp, flip_bit(tp, bit)) for bit in bits]
        + ready(None)
    )
    ready(True)

    def state_copy(u, off):
        to = lax.rem(sp + off, n_sp)
        way = jnp.where(to > sp, 0, 1)
        rows = slice(u * PACK, (u + 1) * PACK)
        sem = off * count + u
        return remote(
            sent.at[way, rows], got.at[off, rows], st_send.at[sem], st_recv.at[sem], (to, tp)
        )

    t_at = lax.broadcasted_iota(jnp.int32, (length, length), 0)
    s_at = lax.broadcasted_iota(jnp.int32, (length, length), 1)
    same = (t_at // BLOCK) == (s_at // BLOCK)
    for u, (q, k, v, g, d, norm, key, per, at) in enumerate(units):
        for way in range(2):
            tri = jnp.where(
                same & ((s_at <= t_at) if way == 0 else (s_at >= t_at)), 1.0, 0.0
            ).astype(jnp.bfloat16)
            cols = slice(at * lanes, (at + 1) * lanes)
            rate = log_sigmoid(d[way, :, cols].astype(jnp.float32)) / TAU
            high = rate.astype(jnp.bfloat16)
            rest = rate - high.astype(jnp.float32)
            mid = rest.astype(jnp.bfloat16)
            low = (rest - mid.astype(jnp.float32)).astype(jnp.bfloat16)
            cum[u] = contract(tri, high, NN) + contract(tri, mid, NN) + contract(tri, low, NN)
            state = jnp.zeros((VALUE_W, lanes), jnp.float32)
            reach = jnp.zeros((1, lanes), jnp.float32)
            lane = lax.broadcasted_iota(jnp.int32, (VALUE_W, lanes), 1) // key
            for n in range(blocks) if way == 0 else range(blocks - 1, -1, -1):
                rows = slice(n * BLOCK, (n + 1) * BLOCK)
                c = cum[u, rows, :]
                e = c[BLOCK - 1 : BLOCK] if way == 0 else c[0:1]
                queries = q[rows, cols].astype(jnp.float32) * key ** (-0.5)
                keys = k[rows, cols].astype(jnp.float32)
                qd[way, u, rows, :] = (queries * jnp.exp(c)).astype(jnp.bfloat16)
                kd[way, u, rows, :] = (keys * jnp.exp(-c)).astype(jnp.bfloat16)
                end = (keys * jnp.exp(e - c)).astype(jnp.bfloat16)
                term = None
                for h in range(per):
                    head = at * per + h
                    value = v[rows, head * VALUE_W : (head + 1) * VALUE_W]
                    new = contract(value, end, TN)
                    term = new if term is None else jnp.where(lane == h, new, term)
                added[way, u, n] = term
                fade = jnp.exp(e)
                ends[way, u, n : n + 1, :] = fade
                state = state * fade + term
                reach = reach + e
            sent[way, u * PACK : u * PACK + VALUE_W, :] = state.astype(jnp.bfloat16)
            sent[way, u * PACK + VALUE_W : (u + 1) * PACK, :] = jnp.broadcast_to(
                jnp.exp(reach), (16, lanes)
            ).astype(jnp.bfloat16)

        @pl.loop(1, n_sp)
        def _(off):
            state_copy(u, off).start()

    sent_states()
    t_blk = lax.broadcasted_iota(jnp.int32, (BLOCK, BLOCK), 0)
    s_blk = lax.broadcasted_iota(jnp.int32, (BLOCK, BLOCK), 1)
    first = 0
    for u, (q, k, v, g, d, norm, key, per, at) in enumerate(units):
        lane = lax.broadcasted_iota(jnp.int32, (BLOCK, lanes), 1) // key
        for h in range(per):
            head = at * per + h
            for n in range(blocks):
                rows = slice(n * BLOCK, (n + 1) * BLOCK)
                scores = None
                for way in range(2):
                    queries = qd[way, u, rows, :]
                    if per > 1:
                        queries = jnp.where(lane == h, queries, jnp.zeros_like(queries))
                    one = contract(queries, kd[way, u, rows, :], NT)
                    one = jnp.where((s_blk <= t_blk) if way == 0 else (s_blk >= t_blk), one, 0.0)
                    scores = one if scores is None else scores + one
                value = v[rows, head * VALUE_W : (head + 1) * VALUE_W]
                total[first + h, rows, :] = contract(scores.astype(jnp.bfloat16), value, NN)
        first += per

    @pl.loop(1, n_sp)
    def _(off):
        for u in range(count):
            state_copy(u, off).wait()

    got_states()
    carried[...] = jnp.zeros_like(carried)

    def fold(way, who):
        off = lax.rem(sp - who + n_sp, n_sp)
        for u in range(count):
            fade = got[off, u * PACK + VALUE_W : (u + 1) * PACK, :][0:1]
            state = got[off, u * PACK : u * PACK + VALUE_W, :]
            carried[way, u] = carried[way, u] * fade.astype(jnp.float32) + state.astype(jnp.float32)

    @pl.loop(0, sp)
    def _(who):
        fold(0, who)

    @pl.loop(0, n_sp - 1 - sp)
    def _(back):
        fold(1, n_sp - 1 - back)

    first = 0
    for u, (q, k, v, g, d, norm, key, per, at) in enumerate(units):
        lane = lax.broadcasted_iota(jnp.int32, (BLOCK, lanes), 1) // key
        for way in range(2):
            state = carried[way, u]
            for n in range(blocks) if way == 0 else range(blocks - 1, -1, -1):
                rows = slice(n * BLOCK, (n + 1) * BLOCK)
                low = state.astype(jnp.bfloat16)
                for h in range(per):
                    queries = qd[way, u, rows, :]
                    if per > 1:
                        queries = jnp.where(lane == h, queries, jnp.zeros_like(queries))
                    total[first + h, rows, :] += contract(queries, low, NT)
                state = state * ends[way, u, n : n + 1, :] + added[way, u, n]
        for h in range(per):
            head = at * per + h
            cols = slice(head * VALUE_W, (head + 1) * VALUE_W)
            x = total[first + h]
            y = x * lax.rsqrt(jnp.mean(x * x, axis=-1, keepdims=True) + EPS) * norm[...]
            gate = g[:, cols].astype(jnp.float32)
            y = y * (gate / (1.0 + jnp.exp(-gate)))
            mixed[:, (first + h) * VALUE_W : (first + h + 1) * VALUE_W] = y.astype(jnp.bfloat16)
        first += per

    rows_dev = res.shape[0]
    split = out1.shape[0]

    def project(mask):
        block = tp
        for bit in bits:
            if mask & bit:
                block = flip_bit(block, bit)
        rows = pl.ds(pl.multiple_of(block * rows_dev, 16), rows_dev)
        return contract(mixed[rows, :split], out1[...], NN) + contract(
            mixed[rows, split:], out2[...], NN
        )

    def part_copy(mask, bit):
        return remote(
            part_send.at[mask],
            part_got.at[mask],
            pt_send.at[mask],
            pt_recv.at[mask],
            (sp, flip_bit(tp, bit)),
        )

    low_bit = lambda m: m & -m
    order = sorted(range(1, n_tp), key=lambda m: (low_bit(m), -m))
    for mask in order:
        bit = low_bit(mask)
        value = project(mask)
        for earlier in bits:
            if earlier < bit:
                part_copy(mask | earlier, earlier).wait_recv()
                value = value + part_got[mask | earlier].astype(jnp.float32)
        part_send[mask] = value.astype(jnp.bfloat16)
        part_copy(mask, bit).start()
    value = project(0)
    for bit in bits:
        part_copy(bit, bit).wait_recv()
        value = value + part_got[bit].astype(jnp.float32)
    stream = (res[...].astype(jnp.float32) + value.astype(jnp.bfloat16).astype(jnp.float32)).astype(
        jnp.bfloat16
    )
    wide = stream.astype(jnp.float32)
    scale = lax.rsqrt(jnp.mean(wide * wide, axis=-1, keepdims=True) + EPS)
    normed = (wide * scale * gain[...]).astype(jnp.bfloat16)
    return stream, normed, [part_copy(mask, low_bit(mask)) for mask in order]


def mix_scratch(n_sp, n_tp, args, residual):
    q1, k1, v1, g1, d1, norm1, out1, q2, k2, v2, g2, d2, norm2, out2 = args
    length = q1.shape[0]
    blocks = length // BLOCK
    count = (q1.shape[1] + q2.shape[1]) // 128
    heads = (v1.shape[1] + v2.shape[1]) // VALUE_W
    rows, width = residual.shape
    packed = count * PACK
    bf, f32 = jnp.bfloat16, jnp.float32
    sem = pltpu.SemaphoreType.DMA
    return [
        pltpu.VMEM((count, length, 128), f32),
        pltpu.VMEM((2, count, length, 128), bf),
        pltpu.VMEM((2, count, length, 128), bf),
        pltpu.VMEM((2, count, blocks, VALUE_W, 128), f32),
        pltpu.VMEM((2, count, -(-blocks // 8) * 8, 128), f32),
        pltpu.VMEM((2, packed, 128), bf),
        pltpu.VMEM((n_sp, packed, 128), bf),
        pltpu.VMEM((2, count, VALUE_W, 128), f32),
        pltpu.VMEM((heads, length, VALUE_W), f32),
        pltpu.VMEM((length, heads * VALUE_W), bf),
        pltpu.VMEM((n_tp, rows, width), bf),
        pltpu.VMEM((n_tp, rows, width), bf),
        sem((n_sp * count,)),
        sem((n_sp * count,)),
        sem((n_tp,)),
        sem((n_tp,)),
    ]


def mix_operands(args, residual, norm_gain):
    q1, k1, v1, g1, d1, norm1, out1, q2, k2, v2, g2, d2, norm2, out2 = args
    return (
        q1, k1, v1, g1, d1, q2, k2, v2, g2, d2,
        norm1[None], norm2[None], out1, out2, residual, norm_gain[None],
    )


def mixer_kernel(n_sp, n_tp, *refs):
    operands, (stream_ref, normed_ref), scratch = refs[:16], refs[16:18], refs[18:]
    ready = lambda go: [] if go is None else None
    stream, normed, pending = mix(n_sp, n_tp, operands, scratch, ready, nothing, nothing)
    stream_ref[...] = stream
    normed_ref[...] = normed
    for one in pending:
        one.wait_send()


def mixer(n_sp, n_tp, args, residual, norm_gain):
    rows, width = residual.shape
    vmem = pl.BlockSpec(memory_space=pltpu.VMEM)
    return pl.pallas_call(
        functools.partial(mixer_kernel, n_sp, n_tp),
        out_shape=(jax.ShapeDtypeStruct((rows, width), jnp.bfloat16),) * 2,
        in_specs=[vmem] * 16,
        out_specs=(vmem, vmem),
        scratch_shapes=mix_scratch(n_sp, n_tp, args, residual),
        compiler_params=pltpu.CompilerParams(
            collective_id=0, has_side_effects=True, vmem_limit_bytes=60 * 2**20
        ),
    )(*mix_operands(args, residual, norm_gain))


def nearest(place, rank):
    half, last = GROUPS // 2, GROUPS - 1
    turned = place // half
    inner = place + turned * (last - 2 * place)
    spot = rank + turned * 0
    if isinstance(rank, int):
        spot = rank + inner * (1 - 2 * rank) if rank < half else rank + 0 * inner
    return spot + turned * (last - 2 * spot)


def rank_of(place, other):
    half, last = GROUPS // 2, GROUPS - 1
    turned = place // half
    inner = place + turned * (last - 2 * place)
    spot = other + turned * (last - 2 * other)
    return spot + inner * (1 - spot // half) * (1 - 2 * spot)


KINDS = 5
COPIES = 10 * GROUPS + 4 * GROUPS + 8


def layer_kernel(n_sp, n_tp, stride, extra, n_scratch, *refs):
    operands = refs[:16]
    weight, slot, w_gate, w_up, w_down, out_ref = refs[16:22]
    scratch = refs[22 : 22 + n_scratch]
    (
        v_gate, v_up, wd, spread, meta_send, meta_got, wslot, z_send, z_extra, data, hid, hgot,
        acc, part, pgot, outs, back_got, kept, w_sem, s_sem, r_sem, zs_sem, zr_sem,
    ) = refs[22 + n_scratch :]
    bf, f32 = jnp.bfloat16, jnp.float32
    sp, tp = lax.axis_index("sp"), lax.axis_index("tp")
    span = stride + extra
    length = GROUPS * stride + extra
    width = data.shape[2]
    units = hid.shape[2]
    place, side = sp // 2, lax.rem(sp, 2)
    core, across, along = (sp, flip_bit(tp, 1)), (sp, flip_bit(tp, 2)), (flip_bit(sp, 1), tp)
    corner = (flip_bit(sp, 1), flip_bit(tp, 2))
    left, right = slice(0, width // 2), slice(width // 2, width)
    far = []
    for i in range(1, GROUPS):
        z = nearest(place, i)
        far.append((i, rank_of(z, place), (z * 2 + side, tp)))
    numbers = iter(range(COPIES))
    started = []

    def copy(source, target, device):
        number = next(numbers)
        return remote(source, target, s_sem.at[number], r_sem.at[number], device)

    def go(one):
        one.start()
        started.append(one)
        return one

    def z_copy(kind, i, rank, source, target, device):
        return remote(
            source,
            target,
            zs_sem.at[kind * GROUPS + i],
            zr_sem.at[kind * GROUPS + rank],
            device,
        )

    loads = [
        pltpu.make_async_copy(source, target, w_sem.at[i])
        for i, (source, target) in enumerate(
            ((w_gate, v_gate), (w_up, v_up), (w_down, wd.at[0]))
        )
    ]
    early = units // 4
    down_y = [
        copy(w_down.at[rows], wd.at[1, rows], along)
        for rows in (slice(0, early), slice(early, units))
    ]
    down_x = copy(w_down, wd.at[2], across)
    upper, lower = slice(0, units // 2), slice(units // 2, units)
    down_yx = copy(wd.at[1, upper], wd.at[3, upper], across)
    down_xy = copy(wd.at[2, lower], wd.at[3, lower], along)
    metas = [
        z_copy(4, i, rank, meta_send.at[slice(i * span, (i + 1) * span)], meta_got.at[rank], to)
        for i, rank, to in far
    ]
    meta_core = copy(wslot.at[0], wslot.at[1], core)

    def block(index):
        return slice(index * span, (index + 1) * span)

    def chunk(o):
        return slice(o * stride, (o + 1) * stride if o < GROUPS - 1 else length)

    def ready(begin):
        if begin is None:
            return [core_peer for core_peer in (corner,)]
        for load in loads:
            load.start()
        go(down_x)
        go(down_y[0])
        rows = slot.shape[1]
        spread[...] = (
            (lax.broadcasted_iota(jnp.int32, (GROUPS * span, rows), 0) == slot[...])
            .astype(f32)
            .astype(bf)
        )
        high = weight[...].astype(bf)
        rest = (weight[...] - high.astype(f32)).astype(bf)
        second = lax.broadcasted_iota(jnp.int32, high.shape, 1) >= 64
        both = jnp.where(second, rest.astype(f32), high.astype(f32)).astype(bf)
        meta_send[...] = contract(spread[...], both, NN).astype(bf)
        for one in metas:
            go(one)

    def sent_states():
        go(down_y[1])

    def meta_wait(o):
        z_copy(4, 0, o, meta_send.at[block(o)], meta_got.at[o], core).wait_recv()

    def got_states():
        own = meta_send[block(0)]
        wslot[0, 0:stride] = own[:stride]
        more = own[stride:].astype(f32)
        for o in range(1, GROUPS):
            meta_wait(o)
            wslot[0, o * stride : (o + 1) * stride] = meta_got[o, :stride]
            more = more + meta_got[o, stride:].astype(f32)
        wslot[0, GROUPS * stride :] = more.astype(bf)
        go(meta_core)

    stream, normed, pending = mix(n_sp, n_tp, operands, scratch, ready, sent_states, got_states)
    kept[...] = stream

    for i, rank, to in far:
        z_send[block(i)] = contract(spread[block(i), :], normed, NN).astype(bf)
        go(
            z_copy(
                0, i, rank,
                z_send.at[slice(i * span, i * span + stride)],
                data.at[0, pl.ds(pl.multiple_of(rank * stride, 16), stride)],
                to,
            )
        )
        go(
            z_copy(
                1, i, rank,
                z_send.at[slice(i * span + stride, (i + 1) * span)],
                z_extra.at[rank],
                to,
            )
        )
    own = contract(spread[block(0), :], normed, NN).astype(bf)
    data[0, chunk(0), :] = own[:stride]
    z_extra[0] = own[stride:]

    flows = []
    for o in range(GROUPS):
        ch = chunk(o)
        flows.append(
            dict(
                a_y=copy(data.at[0, ch, left], data.at[2, ch, left], along),
                b_x=copy(data.at[0, ch, right], data.at[4, ch, right], across),
                a_x=copy(data.at[0, ch, left], data.at[4, ch, left], across),
                b_y=copy(data.at[0, ch, right], data.at[2, ch, right], along),
                c_0=copy(data.at[0, ch], data.at[1, ch], core),
                a_d=copy(data.at[2, ch, left], data.at[6, ch, left], across),
                b_d=copy(data.at[4, ch, right], data.at[6, ch, right], along),
                c_y=copy(data.at[2, ch], data.at[3, ch], core),
                c_x=copy(data.at[4, ch], data.at[5, ch], core),
                c_d=copy(data.at[6, ch], data.at[7, ch], core),
                h_y=copy(hid.at[slice(2, 4), ch], hgot.at[0, :, ch], along),
                h_x=copy(hid.at[slice(4, 6), ch], hgot.at[1, :, ch], across),
                h_d=copy(hid.at[slice(6, 8), ch], hgot.at[2, :, ch], corner),
                p_c=copy(part.at[ch], pgot.at[ch], core),
            )
        )

    def arrive(kind, o, target):
        z_copy(kind, 0, o, target, target, core).wait_recv()

    def stage(o):
        flow = flows[o]
        if o:
            arrive(0, o, data.at[0, slice(o * stride, (o + 1) * stride)])
        if o == GROUPS - 1:
            more = z_extra[0].astype(f32)
            for k in range(1, GROUPS):
                arrive(1, k, z_extra.at[k])
                more = more + z_extra[k].astype(f32)
            data[0, GROUPS * stride :, :] = more.astype(bf)
        for name in ("a_y", "b_x", "a_x", "b_y", "c_0"):
            go(flow[name])

    def forward(o):
        flow = flows[o]
        flow["a_y"].wait_recv()
        go(flow["a_d"])
        flow["b_x"].wait_recv()
        go(flow["b_d"])
        flow["b_y"].wait_recv()
        go(flow["c_y"])
        flow["a_x"].wait_recv()
        go(flow["c_x"])

    def finish(o):
        flow = flows[o]
        flow["a_d"].wait_recv()
        flow["b_d"].wait_recv()
        go(flow["c_d"])

    def compute(o):
        flow, ch = flows[o], chunk(o)
        for name in ("c_0", "c_y", "c_x", "c_d"):
            flow[name].wait_recv()
        n = ch.stop - ch.start

        @pl.loop(0, 2)
        def _(m):
            some = pl.ds(m * 4, 4)
            x = data[some, ch, :].reshape(4 * n, width)
            gate = contract(x, v_gate[...], NN)
            up = contract(x, v_up[...], NN)
            hidden = (gate / (1.0 + jnp.exp(-gate)) * up).astype(bf)
            hid[some, ch, :] = hidden.reshape(4, n, units)

        for name in ("h_y", "h_x", "h_d"):
            go(flow[name])

    lane = lax.broadcasted_iota(jnp.int32, (1, 128), 1)

    def down(o):
        flow, ch = flows[o], chunk(o)
        n = ch.stop - ch.start
        w = wslot[:, ch, :].reshape(2 * n, 128).astype(f32)
        pick = lambda s: jnp.sum(
            jnp.where((lane == s) | (lane == s + 64), w, 0.0), axis=1, keepdims=True
        )
        mine, other = pick(side), pick(1 - side)
        for name in ("h_y", "h_x", "h_d"):
            flow[name].wait_recv()
        tile = 512

        @pl.loop(0, width // tile)
        def _(j):
            cols = pl.ds(pl.multiple_of(j * tile, tile), tile)
            rows = lambda value: value.reshape(2 * n, units)
            a = contract(rows(hid[0:2, ch, :]), wd[0, :, cols], NN) + contract(
                rows(hgot[1, :, ch, :]), wd[2, :, cols], NN
            )
            b = contract(rows(hgot[0, :, ch, :]), wd[1, :, cols], NN) + contract(
                rows(hgot[2, :, ch, :]), wd[3, :, cols], NN
            )
            value = a * mine + b * other
            acc[ch, cols] = value[:n]
            part[ch, cols] = value[n:].astype(bf)

        go(flow["p_c"])

    def give(o):
        flow, ch = flows[o], chunk(o)
        flow["p_c"].wait_recv()
        outs[ch, :] = (acc[ch, :] + pgot[ch, :].astype(f32)).astype(bf)
        rows = slice(o * stride, (o + 1) * stride)
        if o == 0:
            back_got[0:stride] = outs[rows, :]
        else:
            i, rank, to = far[o - 1]
            go(
                z_copy(
                    2, i, rank,
                    outs.at[rows],
                    back_got.at[pl.ds(pl.multiple_of(rank * span, 16), stride)],
                    to,
                )
            )
        if o == GROUPS - 1:
            rows = slice(GROUPS * stride, length)
            back_got[stride:span] = outs[rows, :]
            for i, rank, to in far:
                go(
                    z_copy(
                        3, i, rank,
                        outs.at[rows],
                        back_got.at[pl.ds(pl.multiple_of(rank * span + stride, 16), extra)],
                        to,
                    )
                )

    stage(0)
    down_y[0].wait_recv()
    down_y[1].wait_recv()
    go(down_yx)
    down_x.wait_recv()
    go(down_xy)
    forward(0)
    stage(1)
    for load in loads:
        load.wait()
    meta_core.wait_recv()
    finish(0)
    forward(1)
    compute(0)
    finish(1)
    stage(2)
    down_yx.wait_recv()
    down_xy.wait_recv()
    down(0)
    compute(1)
    give(0)
    forward(2)
    down(1)
    stage(3)
    finish(2)
    give(1)
    compute(2)
    forward(3)
    down(2)
    finish(3)
    give(2)
    compute(3)
    down(3)
    give(3)
    for i in range(1, GROUPS):
        arrive(2, i, back_got.at[slice(i * span, i * span + stride)])
        arrive(3, i, back_got.at[slice(i * span + stride, (i + 1) * span)])
    picked = contract(spread[...], back_got[...], TN)
    out_ref[...] = (kept[...].astype(f32) + picked).astype(bf)
    for one in pending + started:
        one.wait_send()


def whole_layer(n_sp, n_tp, args, residual, norm_gain, routes, weights, capacity, w_gate, w_up, w_down):
    rows, width = residual.shape
    units = w_gate.shape[1]
    stride = capacity // 16 * 16
    over = capacity - stride
    extra = max(16, -(-GROUPS * over // 16) * 16)
    span, length = stride + extra, GROUPS * stride + extra
    place = lax.axis_index("sp") // 2
    group = routes[:, 0] // 2
    position = jnp.arange(rows, dtype=jnp.int32)
    before = (group[:, None] == group[None, :]) & (position[None, :] < position[:, None])
    nth = jnp.sum(before.astype(jnp.int32), axis=1)
    tail = stride + rank_of(group, place) * over + nth - stride
    slot = (rank_of(place, group) * span + jnp.where(nth < stride, nth, tail))[None, :]
    side = routes[:, :, None] % 2 == (jnp.arange(128, dtype=jnp.int32) % 64)[None, None, :]
    weight = jnp.sum(jnp.where(side, weights[:, :, None], 0.0), axis=1)
    bf, f32 = jnp.bfloat16, jnp.float32
    vmem = pl.BlockSpec(memory_space=pltpu.VMEM)
    hbm = pl.BlockSpec(memory_space=pl.ANY)
    sem = pltpu.SemaphoreType.DMA
    mine = mix_scratch(n_sp, n_tp, args, residual)
    return pl.pallas_call(
        functools.partial(layer_kernel, n_sp, n_tp, stride, extra, len(mine)),
        out_shape=jax.ShapeDtypeStruct((rows, width), bf),
        in_specs=[vmem] * 18 + [hbm] * 3,
        out_specs=vmem,
        scratch_shapes=mine
        + [
            pltpu.VMEM(w_gate.shape, bf),
            pltpu.VMEM(w_up.shape, bf),
            pltpu.VMEM((4, units, width), bf),
            pltpu.VMEM((GROUPS * span, rows), bf),
            pltpu.VMEM((GROUPS * span, 128), bf),
            pltpu.VMEM((GROUPS, span, 128), bf),
            pltpu.VMEM((2, length, 128), bf),
            pltpu.VMEM((GROUPS * span, width), bf),
            pltpu.VMEM((GROUPS, extra, width), bf),
            pltpu.VMEM((8, length, width), bf),
            pltpu.VMEM((8, length, units), bf),
            pltpu.VMEM((3, 2, length, units), bf),
            pltpu.VMEM((length, width), f32),
            pltpu.VMEM((length, width), bf),
            pltpu.VMEM((length, width), bf),
            pltpu.VMEM((length, width), bf),
            pltpu.VMEM((GROUPS * span, width), bf),
            pltpu.VMEM((rows, width), bf),
            sem((3,)),
            sem((COPIES,)),
            sem((COPIES,)),
            sem((KINDS * GROUPS,)),
            sem((KINDS * GROUPS,)),
        ],
        compiler_params=pltpu.CompilerParams(
            collective_id=1, has_side_effects=True, vmem_limit_bytes=63 * 2**20
        ),
    )(*mix_operands(args, residual, norm_gain), weight, slot, w_gate, w_up, w_down)


def slot_table(routes, capacity, experts):
    flat = routes.reshape(-1)
    count = flat.shape[0]
    onehot = (flat[:, None] == jnp.arange(experts, dtype=jnp.int32)[None, :]).astype(jnp.int32)
    place = jnp.sum((jnp.cumsum(onehot, axis=0) - onehot) * onehot, axis=1)
    table = (
        jnp.full((experts, capacity), count, jnp.int32)
        .at[flat, place]
        .set(jnp.arange(count, dtype=jnp.int32))
    )
    return (table, place)

def body(
    residual,
    query_one,
    key_one,
    value_one,
    gate_one,
    decay_one,
    norm_one,
    output_one,
    query_two,
    key_two,
    value_two,
    gate_two,
    decay_two,
    norm_two,
    output_two,
    norm_gain,
    expert_ids,
    group_weight,
    pair_weight,
    expert_gate,
    expert_up,
    expert_down,
):
    n_sp, n_tp = lax.axis_size("sp"), lax.axis_size("tp")
    mixing = (
        query_one, key_one, value_one, gate_one, decay_one, norm_one, output_one,
        query_two, key_two, value_two, gate_two, decay_two, norm_two, output_two,
    )
    rows_dev = residual.shape[0]
    rank = lax.axis_index("tp")
    experts = n_sp
    capacity = max(2, 2 * rows_dev // (experts - GROUPS) + 1)
    own_routes = lax.dynamic_slice_in_dim(expert_ids, rank * rows_dev, rows_dev, 0)
    own_group = lax.dynamic_slice_in_dim(group_weight, rank * rows_dev, rows_dev, 0)
    own_pair = lax.dynamic_slice_in_dim(pair_weight, rank * rows_dev, rows_dev, 0)
    weights = own_group[:, None] * own_pair / jnp.sum(own_pair, axis=1, keepdims=True)
    if experts == 2 * GROUPS and n_tp == 4:
        return whole_layer(
            n_sp,
            n_tp,
            mixing,
            residual,
            norm_gain,
            own_routes,
            weights,
            capacity,
            expert_gate[0],
            expert_up[0],
            expert_down[0],
        )
    stream, normed_rows = mixer(n_sp, n_tp, mixing, residual, norm_gain)
    blank = jnp.zeros((1, D), jnp.bfloat16)
    table, own_place = slot_table(own_routes, capacity, experts)
    index = jnp.where(table == 2 * rows_dev, rows_dev, table // 2)
    send = jnp.concatenate([normed_rows, blank], axis=0)[index][None]
    received = lax.all_to_all(send, "sp", split_axis=1, concat_axis=1, tiled=True)
    received = lax.all_gather(received, "tp", axis=0, tiled=True)
    flat = received.reshape(-1, received.shape[-1])
    gate_part = jnp.dot(flat, expert_gate[0], preferred_element_type=jnp.float32)
    up_part = jnp.dot(flat, expert_up[0], preferred_element_type=jnp.float32)
    hidden = (jax.nn.silu(gate_part) * up_part).astype(jnp.bfloat16)
    share_sum = lax.psum_scatter(
        jnp.dot(hidden, expert_down[0], preferred_element_type=jnp.float32)
        .reshape(received.shape)
        .astype(jnp.bfloat16),
        "tp",
        scatter_dimension=0,
        tiled=True,
    )
    returned = lax.all_to_all(share_sum, "sp", split_axis=1, concat_axis=1, tiled=True)
    slot_index = own_routes.reshape(-1) * capacity + own_place
    picked = returned.reshape(-1, D)[slot_index].astype(jnp.float32).reshape(rows_dev, 2, D)
    layer = stream.astype(jnp.float32) + jnp.sum(weights[:, :, None] * picked, axis=1)
    return layer.astype(jnp.bfloat16)

def solution(mesh):
    placed = (
        P(("sp", "tp"), None),
        P("sp", "tp"),
        P("sp", "tp"),
        P("sp", "tp"),
        P("sp", "tp"),
        P(None, "sp", "tp"),
        P(),
        P("tp", None),
        P("sp", "tp"),
        P("sp", "tp"),
        P("sp", "tp"),
        P("sp", "tp"),
        P(None, "sp", "tp"),
        P(),
        P("tp", None),
        P(),
        P("sp", None),
        P("sp"),
        P("sp", None),
        P("sp", None, "tp"),
        P("sp", None, "tp"),
        P("sp", "tp", None),
    )
    return jax.shard_map(
        body, mesh=mesh, in_specs=placed, out_specs=P(("sp", "tp"), None), check_vma=False
    )
```

```python
import functools

import jax
import jax.numpy as jnp
from jax import lax
from jax.experimental import pallas as pl
from jax.experimental.pallas import tpu as pltpu
from jax.sharding import PartitionSpec as P

D = 2048
KEY_ONE = 64
KEY_TWO = 128
VALUE_W = 128
BLOCK = 64
GROUPS = 4


MESH = pl.DeviceIdType.MESH
TAU = 16.0
EPS = 1e-06


def log_sigmoid(x):
    return jnp.minimum(x, 0.0) - jnp.log1p(jnp.exp(-jnp.abs(x)))


def contract(a, b, dims):
    return lax.dot_general(a, b, (dims, ((), ())), preferred_element_type=jnp.float32)


NN, NT, TN = ((1,), (0,)), ((1,), (1,)), ((0,), (0,))


def flip_bit(index, bit):
    return index + bit - 2 * bit * lax.rem(index // bit, 2)


def meet(peers):
    barrier = pltpu.get_barrier_semaphore()
    for peer in peers:
        pl.semaphore_signal(barrier, inc=1, device_id=peer, device_id_type=MESH)
    pl.semaphore_wait(barrier, len(peers))


def remote(source, target, send, recv, device):
    return pltpu.make_async_remote_copy(
        src_ref=source,
        dst_ref=target,
        send_sem=send,
        recv_sem=recv,
        device_id=device,
        device_id_type=MESH,
    )


def nothing(*_):
    return None


PACK = VALUE_W + 16


def mix(n_sp, n_tp, operands, scratch, ready, sent_states, got_states):
    q1, k1, v1, g1, d1, q2, k2, v2, g2, d2, norm1, norm2, out1, out2, res, gain = operands
    cum, qd, kd, added, ends, sent, got, carried, total, mixed, part_send, part_got = scratch[:12]
    fade_own, fade_all, half_send, half_got = scratch[12:16]
    st_send, st_recv, pt_send, pt_recv, fd_send, fd_recv, hf_send, hf_recv = scratch[16:]
    sp, tp = lax.axis_index("sp"), lax.axis_index("tp")
    length = q1.shape[0]
    blocks = length // BLOCK
    lanes = 128
    units = []
    for q, k, v, g, d, norm, key in (
        (q1, k1, v1, g1, d1, norm1, KEY_ONE),
        (q2, k2, v2, g2, d2, norm2, KEY_TWO),
    ):
        per = lanes // key
        for at in range(q.shape[1] // lanes):
            units.append((q, k, v, g, d, norm, key, per, at))
    count = len(units)
    bits = [1 << r for r in range(n_tp.bit_length() - 1)]
    paired = n_sp == 2 * GROUPS
    place, side = sp // 2, lax.rem(sp, 2)
    mate = (flip_bit(sp, 1), tp)

    meet(
        [(lax.rem(sp + off, n_sp), tp) for off in range(1, n_sp)]
        + [(sp, flip_bit(tp, bit)) for bit in bits]
        + ready(None)
    )
    ready(True)

    def state_copy(u, off):
        to = lax.rem(sp + off, n_sp)
        way = jnp.where(to > sp, 0, 1)
        rows = slice(u * PACK, (u + 1) * PACK)
        sem = off * count + u
        return remote(
            sent.at[way, rows], got.at[off, rows], st_send.at[sem], st_recv.at[sem], (to, tp)
        )

    def place_copy(u, off):
        z = lax.rem(place + off, GROUPS)
        way = jnp.where(z > place, 0, 1) if off else side
        rows = slice(u * PACK, u * PACK + VALUE_W)
        sem = off * count + u
        return remote(
            sent.at[way, rows],
            got.at[off, rows],
            st_send.at[sem],
            st_recv.at[sem],
            (z * 2 + side, tp) if off else mate,
        )

    def fade_copy(off):
        to = (lax.rem(sp + off, n_sp), tp)
        return remote(fade_own, fade_all.at[off], fd_send.at[off], fd_recv.at[off], to)

    def half_copy(u):
        return remote(half_send.at[u], half_got.at[u], hf_send.at[u], hf_recv.at[u], mate)

    t_at = lax.broadcasted_iota(jnp.int32, (length, length), 0)
    s_at = lax.broadcasted_iota(jnp.int32, (length, length), 1)
    same = (t_at // BLOCK) == (s_at // BLOCK)
    for u, (q, k, v, g, d, norm, key, per, at) in enumerate(units):
        for way in range(2):
            tri = jnp.where(
                same & ((s_at <= t_at) if way == 0 else (s_at >= t_at)), 1.0, 0.0
            ).astype(jnp.bfloat16)
            cols = slice(at * lanes, (at + 1) * lanes)
            rate = log_sigmoid(d[way, :, cols].astype(jnp.float32)) / TAU
            high = rate.astype(jnp.bfloat16)
            rest = rate - high.astype(jnp.float32)
            mid = rest.astype(jnp.bfloat16)
            low = (rest - mid.astype(jnp.float32)).astype(jnp.bfloat16)
            cum[u] = contract(tri, high, NN) + contract(tri, mid, NN) + contract(tri, low, NN)
            state = jnp.zeros((VALUE_W, lanes), jnp.float32)
            reach = jnp.zeros((1, lanes), jnp.float32)
            lane = lax.broadcasted_iota(jnp.int32, (VALUE_W, lanes), 1) // key
            for n in range(blocks) if way == 0 else range(blocks - 1, -1, -1):
                rows = slice(n * BLOCK, (n + 1) * BLOCK)
                c = cum[u, rows, :]
                e = c[BLOCK - 1 : BLOCK] if way == 0 else c[0:1]
                queries = q[rows, cols].astype(jnp.float32) * key ** (-0.5)
                keys = k[rows, cols].astype(jnp.float32)
                qd[way, u, rows, :] = (queries * jnp.exp(c)).astype(jnp.bfloat16)
                kd[way, u, rows, :] = (keys * jnp.exp(-c)).astype(jnp.bfloat16)
                end = (keys * jnp.exp(e - c)).astype(jnp.bfloat16)
                term = None
                for h in range(per):
                    head = at * per + h
                    value = v[rows, head * VALUE_W : (head + 1) * VALUE_W]
                    new = contract(value, end, TN)
                    term = new if term is None else jnp.where(lane == h, new, term)
                added[way, u, n] = term
                fade = jnp.exp(e)
                ends[way, u, n : n + 1, :] = fade
                state = state * fade + term
                reach = reach + e
            sent[way, u * PACK : u * PACK + VALUE_W, :] = state.astype(jnp.bfloat16)
            if paired:
                row = way * count + u
                fade_own[row : row + 1, :] = jnp.exp(reach)
            else:
                sent[way, u * PACK + VALUE_W : (u + 1) * PACK, :] = jnp.broadcast_to(
                    jnp.exp(reach), (16, lanes)
                ).astype(jnp.bfloat16)

        if paired:
            for off in (1, 2, 3, 0):
                place_copy(u, off).start()
        else:

            @pl.loop(1, n_sp)
            def _(off):
                state_copy(u, off).start()

    if paired:

        @pl.loop(1, n_sp)
        def _(off):
            fade_copy(off).start()

    sent_states()
    t_blk = lax.broadcasted_iota(jnp.int32, (BLOCK, BLOCK), 0)
    s_blk = lax.broadcasted_iota(jnp.int32, (BLOCK, BLOCK), 1)
    first = 0
    for u, (q, k, v, g, d, norm, key, per, at) in enumerate(units):
        lane = lax.broadcasted_iota(jnp.int32, (BLOCK, lanes), 1) // key
        for h in range(per):
            head = at * per + h
            for n in range(blocks):
                rows = slice(n * BLOCK, (n + 1) * BLOCK)
                scores = None
                for way in range(2):
                    queries = qd[way, u, rows, :]
                    if per > 1:
                        queries = jnp.where(lane == h, queries, jnp.zeros_like(queries))
                    one = contract(queries, kd[way, u, rows, :], NT)
                    one = jnp.where((s_blk <= t_blk) if way == 0 else (s_blk >= t_blk), one, 0.0)
                    scores = one if scores is None else scores + one
                value = v[rows, head * VALUE_W : (head + 1) * VALUE_W]
                total[first + h, rows, :] = contract(scores.astype(jnp.bfloat16), value, NN)
        first += per

    carried[...] = jnp.zeros_like(carried)

    def fold(way, who):
        off = lax.rem(sp - who + n_sp, n_sp)
        for u in range(count):
            fade = got[off, u * PACK + VALUE_W : (u + 1) * PACK, :][0:1]
            state = got[off, u * PACK : u * PACK + VALUE_W, :]
            carried[way, u] = carried[way, u] * fade.astype(jnp.float32) + state.astype(jnp.float32)

    def fade_of(who, way, u):
        row = way * count + u
        return fade_all[lax.rem(sp - who + n_sp, n_sp), row : row + 1, :]

    def fold_place(way, u, z):
        off = lax.rem(place - z + GROUPS, GROUPS)
        fades = [fade_of(2 * z + y, way, u) for y in range(2)]
        state = got[off, u * PACK : u * PACK + VALUE_W, :].astype(jnp.float32)
        later = jnp.where(side == way, fades[1 - way], jnp.ones_like(fades[0]))
        carried[way, u] = carried[way, u] * (fades[0] * fades[1]) + state * later

    if paired:

        @pl.loop(1, n_sp)
        def _(off):
            fade_copy(off).wait()

        for u in range(count):
            for off in range(1, GROUPS):
                place_copy(u, off).wait()

            @pl.loop(0, place)
            def _(z):
                fold_place(0, u, z)

            @pl.loop(0, GROUPS - 1 - place)
            def _(back):
                fold_place(1, u, GROUPS - 1 - back)

            half_send[u] = carried[:, u].astype(jnp.bfloat16)
            half_copy(u).start()
        got_states()
        for u in range(count):
            place_copy(u, 0).wait()
            half_copy(u).wait()
            carried[:, u] = carried[:, u] + half_got[u].astype(jnp.float32)
            way = 1 - side
            off = 1 + way * (n_sp - 2)
            fade = fade_all[off, pl.ds(way * count + u, 1), :]
            state = got[0, u * PACK : u * PACK + VALUE_W, :].astype(jnp.float32)
            carried[way, u] = carried[way, u] * fade + state
    else:

        @pl.loop(1, n_sp)
        def _(off):
            for u in range(count):
                state_copy(u, off).wait()

        @pl.loop(0, sp)
        def _(who):
            fold(0, who)

        @pl.loop(0, n_sp - 1 - sp)
        def _(back):
            fold(1, n_sp - 1 - back)

    first = 0
    for u, (q, k, v, g, d, norm, key, per, at) in enumerate(units):
        lane = lax.broadcasted_iota(jnp.int32, (BLOCK, lanes), 1) // key
        for way in range(2):
            state = carried[way, u]
            for n in range(blocks) if way == 0 else range(blocks - 1, -1, -1):
                rows = slice(n * BLOCK, (n + 1) * BLOCK)
                low = state.astype(jnp.bfloat16)
                for h in range(per):
                    queries = qd[way, u, rows, :]
                    if per > 1:
                        queries = jnp.where(lane == h, queries, jnp.zeros_like(queries))
                    total[first + h, rows, :] += contract(queries, low, NT)
                state = state * ends[way, u, n : n + 1, :] + added[way, u, n]
        for h in range(per):
            head = at * per + h
            cols = slice(head * VALUE_W, (head + 1) * VALUE_W)
            x = total[first + h]
            y = x * lax.rsqrt(jnp.mean(x * x, axis=-1, keepdims=True) + EPS) * norm[...]
            gate = g[:, cols].astype(jnp.float32)
            y = y * (gate / (1.0 + jnp.exp(-gate)))
            mixed[:, (first + h) * VALUE_W : (first + h + 1) * VALUE_W] = y.astype(jnp.bfloat16)
        first += per

    rows_dev = res.shape[0]
    split = out1.shape[0]

    def project(mask):
        block = tp
        for bit in bits:
            if mask & bit:
                block = flip_bit(block, bit)
        rows = pl.ds(pl.multiple_of(block * rows_dev, 16), rows_dev)
        return contract(mixed[rows, :split], out1[...], NN) + contract(
            mixed[rows, split:], out2[...], NN
        )

    def part_copy(mask, bit):
        return remote(
            part_send.at[mask],
            part_got.at[mask],
            pt_send.at[mask],
            pt_recv.at[mask],
            (sp, flip_bit(tp, bit)),
        )

    low_bit = lambda m: m & -m
    order = sorted(range(1, n_tp), key=lambda m: (low_bit(m), -m))
    for mask in order:
        bit = low_bit(mask)
        value = project(mask)
        for earlier in bits:
            if earlier < bit:
                part_copy(mask | earlier, earlier).wait_recv()
                value = value + part_got[mask | earlier].astype(jnp.float32)
        part_send[mask] = value.astype(jnp.bfloat16)
        part_copy(mask, bit).start()
    value = project(0)
    for bit in bits:
        part_copy(bit, bit).wait_recv()
        value = value + part_got[bit].astype(jnp.float32)
    stream = (res[...].astype(jnp.float32) + value.astype(jnp.bfloat16).astype(jnp.float32)).astype(
        jnp.bfloat16
    )
    wide = stream.astype(jnp.float32)
    scale = lax.rsqrt(jnp.mean(wide * wide, axis=-1, keepdims=True) + EPS)
    normed = (wide * scale * gain[...]).astype(jnp.bfloat16)
    return stream, normed, [part_copy(mask, low_bit(mask)) for mask in order]


def mix_scratch(n_sp, n_tp, args, residual):
    q1, k1, v1, g1, d1, norm1, out1, q2, k2, v2, g2, d2, norm2, out2 = args
    length = q1.shape[0]
    blocks = length // BLOCK
    count = (q1.shape[1] + q2.shape[1]) // 128
    heads = (v1.shape[1] + v2.shape[1]) // VALUE_W
    rows, width = residual.shape
    packed = count * PACK
    bf, f32 = jnp.bfloat16, jnp.float32
    sem = pltpu.SemaphoreType.DMA
    return [
        pltpu.VMEM((count, length, 128), f32),
        pltpu.VMEM((2, count, length, 128), bf),
        pltpu.VMEM((2, count, length, 128), bf),
        pltpu.VMEM((2, count, blocks, VALUE_W, 128), f32),
        pltpu.VMEM((2, count, -(-blocks // 8) * 8, 128), f32),
        pltpu.VMEM((2, packed, 128), bf),
        pltpu.VMEM((n_sp, packed, 128), bf),
        pltpu.VMEM((2, count, VALUE_W, 128), f32),
        pltpu.VMEM((heads, length, VALUE_W), f32),
        pltpu.VMEM((length, heads * VALUE_W), bf),
        pltpu.VMEM((n_tp, rows, width), bf),
        pltpu.VMEM((n_tp, rows, width), bf),
        pltpu.VMEM((-(-2 * count // 8) * 8, 128), f32),
        pltpu.VMEM((n_sp, -(-2 * count // 8) * 8, 128), f32),
        pltpu.VMEM((count, 2, VALUE_W, 128), bf),
        pltpu.VMEM((count, 2, VALUE_W, 128), bf),
        sem((n_sp * count,)),
        sem((n_sp * count,)),
        sem((n_tp,)),
        sem((n_tp,)),
        sem((n_sp,)),
        sem((n_sp,)),
        sem((count,)),
        sem((count,)),
    ]


def mix_operands(args, residual, norm_gain):
    q1, k1, v1, g1, d1, norm1, out1, q2, k2, v2, g2, d2, norm2, out2 = args
    return (
        q1, k1, v1, g1, d1, q2, k2, v2, g2, d2,
        norm1[None], norm2[None], out1, out2, residual, norm_gain[None],
    )


def mixer_kernel(n_sp, n_tp, *refs):
    operands, (stream_ref, normed_ref), scratch = refs[:16], refs[16:18], refs[18:]
    ready = lambda go: [] if go is None else None
    stream, normed, pending = mix(n_sp, n_tp, operands, scratch, ready, nothing, nothing)
    stream_ref[...] = stream
    normed_ref[...] = normed
    for one in pending:
        one.wait_send()


def mixer(n_sp, n_tp, args, residual, norm_gain):
    rows, width = residual.shape
    vmem = pl.BlockSpec(memory_space=pltpu.VMEM)
    return pl.pallas_call(
        functools.partial(mixer_kernel, n_sp, n_tp),
        out_shape=(jax.ShapeDtypeStruct((rows, width), jnp.bfloat16),) * 2,
        in_specs=[vmem] * 16,
        out_specs=(vmem, vmem),
        scratch_shapes=mix_scratch(n_sp, n_tp, args, residual),
        compiler_params=pltpu.CompilerParams(
            collective_id=0, has_side_effects=True, vmem_limit_bytes=60 * 2**20
        ),
    )(*mix_operands(args, residual, norm_gain))


def nearest(place, rank):
    half, last = GROUPS // 2, GROUPS - 1
    turned = place // half
    inner = place + turned * (last - 2 * place)
    spot = rank + turned * 0
    if isinstance(rank, int):
        spot = rank + inner * (1 - 2 * rank) if rank < half else rank + 0 * inner
    return spot + turned * (last - 2 * spot)


def rank_of(place, other):
    half, last = GROUPS // 2, GROUPS - 1
    turned = place // half
    inner = place + turned * (last - 2 * place)
    spot = other + turned * (last - 2 * other)
    return spot + inner * (1 - spot // half) * (1 - 2 * spot)


KINDS = 5
COPIES = 10 * GROUPS + 4 * GROUPS + 8


def layer_kernel(n_sp, n_tp, stride, over, extra, n_scratch, *refs):
    operands = refs[:16]
    ids, group_share, pair_share, w_gate, w_up, w_down, out_ref = refs[16:23]
    scratch = refs[23 : 23 + n_scratch]
    (
        v_gate, v_up, wd, spread, meta_send, meta_got, wslot, z_send, z_extra, data, hid, hgot,
        acc, part, pgot, outs, back_got, kept, w_sem, s_sem, r_sem, zs_sem, zr_sem,
    ) = refs[23 + n_scratch :]
    bf, f32 = jnp.bfloat16, jnp.float32
    sp, tp = lax.axis_index("sp"), lax.axis_index("tp")
    span = stride + extra
    length = GROUPS * stride + extra
    wire = -(-GROUPS * over // 8) * 8
    width = data.shape[2]
    units = hid.shape[2]
    place, side = sp // 2, lax.rem(sp, 2)
    core, across, along = (sp, flip_bit(tp, 1)), (sp, flip_bit(tp, 2)), (flip_bit(sp, 1), tp)
    corner = (flip_bit(sp, 1), flip_bit(tp, 2))
    left, right = slice(0, width // 2), slice(width // 2, width)
    far = []
    for i in range(1, GROUPS):
        z = nearest(place, i)
        far.append((i, rank_of(z, place), (z * 2 + side, tp)))
    numbers = iter(range(COPIES))
    started = []

    def copy(source, target, device):
        number = next(numbers)
        return remote(source, target, s_sem.at[number], r_sem.at[number], device)

    def go(one):
        one.start()
        started.append(one)
        return one

    def z_copy(kind, i, rank, source, target, device):
        return remote(
            source,
            target,
            zs_sem.at[kind * GROUPS + i],
            zr_sem.at[kind * GROUPS + rank],
            device,
        )

    loads = [
        pltpu.make_async_copy(source, target, w_sem.at[i])
        for i, (source, target) in enumerate(
            ((w_gate, v_gate), (w_up, v_up), (w_down, wd.at[0]))
        )
    ]
    early = units // 2
    down_y = [
        copy(w_down.at[rows], wd.at[1, rows], along)
        for rows in (slice(0, early), slice(early, units))
    ]
    down_x = copy(w_down, wd.at[2], across)
    upper, lower = slice(0, units // 2), slice(units // 2, units)
    down_yx = copy(wd.at[1, upper], wd.at[3, upper], across)
    down_xy = copy(wd.at[2, lower], wd.at[3, lower], along)
    metas = [
        z_copy(4, i, rank, meta_send.at[slice(i * span, (i + 1) * span)], meta_got.at[rank], to)
        for i, rank, to in far
    ]
    meta_core = copy(wslot.at[0], wslot.at[1], core)

    def block(index):
        return slice(index * span, (index + 1) * span)

    def chunk(o):
        return slice(o * stride, (o + 1) * stride if o < GROUPS - 1 else length)

    def moved(o):
        return slice(o * stride, (o + 1) * stride if o < GROUPS - 1 else GROUPS * stride + wire)

    def routing():
        rows, tokens = spread.shape[1], ids.shape[1]
        first, share = ids[0:1, :], group_share[...]
        kind = lax.broadcasted_iota(jnp.int32, (8, 1), 0)
        member = ((first >= 2 * kind) & (first < 2 * kind + 2)).astype(f32)
        from_at = lax.broadcasted_iota(jnp.int32, (tokens, tokens), 0)
        to_at = lax.broadcasted_iota(jnp.int32, (tokens, tokens), 1)
        before = jnp.where((from_at < to_at) & (from_at // rows == to_at // rows), 1.0, 0.0)
        counts = contract(member.astype(bf), before.astype(bf), NN)
        nth = jnp.sum(member * counts, axis=0, keepdims=True)
        named = lax.rem(kind, GROUPS)
        base = (rank_of(place, named) * span).astype(f32)
        shift = (rank_of(named, place) * over).astype(f32)
        seat = base + jnp.where(nth < stride, nth, nth + shift)
        seat = jnp.sum(member * seat, axis=0, keepdims=True)
        pair = pair_share[0:1, :] + pair_share[1:2, :]
        w_first = share * pair_share[0:1, :] / pair
        w_second = share * pair_share[1:2, :] / pair
        even = lax.rem(first, 2) == 0
        table = jnp.zeros((8, tokens), f32)
        table = jnp.where(kind == 0, seat, table)
        for s in range(2):
            w = jnp.where(even, w_first, w_second) if s == 0 else jnp.where(even, w_second, w_first)
            high = w.astype(bf).astype(f32)
            table = jnp.where(kind == 1 + s, high, table)
            table = jnp.where(kind == 3 + s, w - high, table)
        at = lax.broadcasted_iota(jnp.int32, (tokens, rows), 0)
        own_at = lax.broadcasted_iota(jnp.int32, (tokens, rows), 1) + tp * rows
        select = jnp.where(at == own_at, 1.0, 0.0).astype(bf)
        table = contract(table.astype(bf), select, NN)
        seats = lax.broadcasted_iota(jnp.int32, (GROUPS * span, rows), 0)
        spread[...] = jnp.where(seats == table[0:1].astype(jnp.int32), 1.0, 0.0).astype(bf)
        line = lax.broadcasted_iota(jnp.int32, (128, 1), 0)
        lines = jnp.zeros((128, rows), f32)
        for row, spot in ((1, 0), (2, 1), (3, 64), (4, 65)):
            lines = jnp.where(line == spot, table[row : row + 1], lines)
        meta_send[...] = contract(spread[...], lines.astype(bf), NT).astype(bf)

    def ready(begin):
        if begin is None:
            return [corner]
        for load in loads:
            load.start()
        rest = slice(GROUPS * stride + wire, length)
        if wire < extra:
            data[:, rest, :] = jnp.zeros((8, extra - wire, width), bf)
            hgot[:, :, rest, :] = jnp.zeros((3, 2, extra - wire, units), bf)
            pgot[rest, :] = jnp.zeros((extra - wire, width), bf)
            for i in range(GROUPS):
                spare = slice(i * span + stride + wire, (i + 1) * span)
                back_got[spare, :] = jnp.zeros((extra - wire, width), bf)
        go(down_x)
        go(down_y[0])
        routing()
        for one in metas:
            go(one)

    def sent_states():
        go(down_y[1])

    def meta_wait(o):
        z_copy(4, 0, o, meta_send.at[block(o)], meta_got.at[o], core).wait_recv()

    def got_states():
        own = meta_send[block(0)]
        wslot[0, 0:stride] = own[:stride]
        more = own[stride:].astype(f32)
        for o in range(1, GROUPS):
            meta_wait(o)
            wslot[0, o * stride : (o + 1) * stride] = meta_got[o, :stride]
            more = more + meta_got[o, stride:].astype(f32)
        wslot[0, GROUPS * stride :] = more.astype(bf)
        go(meta_core)

    stream, normed, pending = mix(n_sp, n_tp, operands, scratch, ready, sent_states, got_states)
    kept[...] = stream

    for i, rank, to in far:
        z_send[block(i)] = contract(spread[block(i), :], normed, NN).astype(bf)
        go(
            z_copy(
                0, i, rank,
                z_send.at[slice(i * span, i * span + stride)],
                data.at[0, pl.ds(pl.multiple_of(rank * stride, 16), stride)],
                to,
            )
        )
        go(
            z_copy(
                1, i, rank,
                z_send.at[slice(i * span + stride, i * span + stride + wire)],
                z_extra.at[rank],
                to,
            )
        )
    own = contract(spread[block(0), :], normed, NN).astype(bf)
    data[0, chunk(0), :] = own[:stride]
    z_extra[0] = own[stride : stride + wire]

    flows = []
    for o in range(GROUPS):
        ch = moved(o)
        flows.append(
            dict(
                a_y=copy(data.at[0, ch, left], data.at[2, ch, left], along),
                b_x=copy(data.at[0, ch, right], data.at[4, ch, right], across),
                a_x=copy(data.at[0, ch, left], data.at[4, ch, left], across),
                b_y=copy(data.at[0, ch, right], data.at[2, ch, right], along),
                c_0=copy(data.at[0, ch], data.at[1, ch], core),
                a_d=copy(data.at[2, ch, left], data.at[6, ch, left], across),
                b_d=copy(data.at[4, ch, right], data.at[6, ch, right], along),
                c_y=copy(data.at[2, ch], data.at[3, ch], core),
                c_x=copy(data.at[4, ch], data.at[5, ch], core),
                c_d=copy(data.at[6, ch], data.at[7, ch], core),
                h_y=copy(hid.at[slice(2, 4), ch], hgot.at[0, :, ch], along),
                h_x=copy(hid.at[slice(4, 6), ch], hgot.at[1, :, ch], across),
                h_d=copy(hid.at[slice(6, 8), ch], hgot.at[2, :, ch], corner),
                p_c=copy(part.at[ch], pgot.at[ch], core),
            )
        )

    def arrive(kind, o, target):
        z_copy(kind, 0, o, target, target, core).wait_recv()

    def stage(o):
        flow = flows[o]
        if o:
            arrive(0, o, data.at[0, slice(o * stride, (o + 1) * stride)])
        if o == GROUPS - 1:
            more = z_extra[0].astype(f32)
            for k in range(1, GROUPS):
                arrive(1, k, z_extra.at[k])
                more = more + z_extra[k].astype(f32)
            data[0, GROUPS * stride : GROUPS * stride + wire, :] = more.astype(bf)
        for name in ("a_y", "b_x", "a_x", "b_y", "c_0"):
            go(flow[name])

    def forward(o):
        flow = flows[o]
        flow["a_y"].wait_recv()
        go(flow["a_d"])
        flow["b_x"].wait_recv()
        go(flow["b_d"])
        flow["b_y"].wait_recv()
        go(flow["c_y"])
        flow["a_x"].wait_recv()
        go(flow["c_x"])

    def finish(o):
        flow = flows[o]
        flow["a_d"].wait_recv()
        flow["b_d"].wait_recv()
        go(flow["c_d"])

    def compute(o):
        flow, ch = flows[o], chunk(o)
        for name in ("c_0", "c_y", "c_x", "c_d"):
            flow[name].wait_recv()
        n = ch.stop - ch.start

        @pl.loop(0, 2)
        def _(m):
            some = pl.ds(m * 4, 4)
            x = data[some, ch, :].reshape(4 * n, width)
            gate = contract(x, v_gate[...], NN)
            up = contract(x, v_up[...], NN)
            hidden = (gate / (1.0 + jnp.exp(-gate)) * up).astype(bf)
            hid[some, ch, :] = hidden.reshape(4, n, units)

        for name in ("h_y", "h_x", "h_d"):
            go(flow[name])

    lane = lax.broadcasted_iota(jnp.int32, (1, 128), 1)

    def down(o):
        flow, ch = flows[o], chunk(o)
        n = ch.stop - ch.start
        w = wslot[:, ch, :].reshape(2 * n, 128).astype(f32)
        pick = lambda s: jnp.sum(
            jnp.where((lane == s) | (lane == s + 64), w, 0.0), axis=1, keepdims=True
        )
        mine, other = pick(side), pick(1 - side)
        for name in ("h_y", "h_x", "h_d"):
            flow[name].wait_recv()
        tile = 512

        @pl.loop(0, width // tile)
        def _(j):
            cols = pl.ds(pl.multiple_of(j * tile, tile), tile)
            rows = lambda value: value.reshape(2 * n, units)
            a = contract(rows(hid[0:2, ch, :]), wd[0, :, cols], NN) + contract(
                rows(hgot[1, :, ch, :]), wd[2, :, cols], NN
            )
            b = contract(rows(hgot[0, :, ch, :]), wd[1, :, cols], NN) + contract(
                rows(hgot[2, :, ch, :]), wd[3, :, cols], NN
            )
            value = a * mine + b * other
            acc[ch, cols] = value[:n]
            part[ch, cols] = value[n:].astype(bf)

        go(flow["p_c"])

    def give(o):
        flow, ch = flows[o], chunk(o)
        flow["p_c"].wait_recv()
        outs[ch, :] = (acc[ch, :] + pgot[ch, :].astype(f32)).astype(bf)
        rows = slice(o * stride, (o + 1) * stride)
        if o == 0:
            back_got[0:stride] = outs[rows, :]
        else:
            i, rank, to = far[o - 1]
            go(
                z_copy(
                    2, i, rank,
                    outs.at[rows],
                    back_got.at[pl.ds(pl.multiple_of(rank * span, 16), stride)],
                    to,
                )
            )
        if o == GROUPS - 1:
            rows = slice(GROUPS * stride, GROUPS * stride + wire)
            back_got[stride : stride + wire] = outs[rows, :]
            for i, rank, to in far:
                go(
                    z_copy(
                        3, i, rank,
                        outs.at[rows],
                        back_got.at[pl.ds(pl.multiple_of(rank * span + stride, 16), wire)],
                        to,
                    )
                )

    stage(0)
    forward(0)
    stage(1)
    for load in loads:
        load.wait()
    finish(0)
    compute(0)
    forward(1)
    down_y[0].wait_recv()
    down_y[1].wait_recv()
    go(down_yx)
    down_x.wait_recv()
    go(down_xy)
    stage(2)
    finish(1)
    compute(1)
    forward(2)
    stage(3)
    meta_core.wait_recv()
    down_yx.wait_recv()
    down_xy.wait_recv()
    down(0)
    finish(2)
    compute(2)
    down(1)
    forward(3)
    give(0)
    give(1)
    down(2)
    finish(3)
    compute(3)
    give(2)
    down(3)
    give(3)
    for i in range(1, GROUPS):
        arrive(2, i, back_got.at[slice(i * span, i * span + stride)])
        arrive(3, i, back_got.at[slice(i * span + stride, i * span + stride + wire)])
    picked = contract(spread[...], back_got[...], TN)
    out_ref[...] = (kept[...].astype(f32) + picked).astype(bf)
    for one in pending + started:
        one.wait_send()


def whole_layer(n_sp, n_tp, args, residual, norm_gain, routing, capacity, w_gate, w_up, w_down):
    rows, width = residual.shape
    units = w_gate.shape[1]
    stride = capacity // 16 * 16
    over = capacity - stride
    extra = max(16, -(-GROUPS * over // 16) * 16)
    span, length = stride + extra, GROUPS * stride + extra
    bf, f32 = jnp.bfloat16, jnp.float32
    vmem = pl.BlockSpec(memory_space=pltpu.VMEM)
    hbm = pl.BlockSpec(memory_space=pl.ANY)
    sem = pltpu.SemaphoreType.DMA
    mine = mix_scratch(n_sp, n_tp, args, residual)
    return pl.pallas_call(
        functools.partial(layer_kernel, n_sp, n_tp, stride, over, extra, len(mine)),
        out_shape=jax.ShapeDtypeStruct((rows, width), bf),
        in_specs=[vmem] * 19 + [hbm] * 3,
        out_specs=vmem,
        scratch_shapes=mine
        + [
            pltpu.VMEM(w_gate.shape, bf),
            pltpu.VMEM(w_up.shape, bf),
            pltpu.VMEM((4, units, width), bf),
            pltpu.VMEM((GROUPS * span, rows), bf),
            pltpu.VMEM((GROUPS * span, 128), bf),
            pltpu.VMEM((GROUPS, span, 128), bf),
            pltpu.VMEM((2, length, 128), bf),
            pltpu.VMEM((GROUPS * span, width), bf),
            pltpu.VMEM((GROUPS, -(-GROUPS * over // 8) * 8, width), bf),
            pltpu.VMEM((8, length, width), bf),
            pltpu.VMEM((8, length, units), bf),
            pltpu.VMEM((3, 2, length, units), bf),
            pltpu.VMEM((length, width), f32),
            pltpu.VMEM((length, width), bf),
            pltpu.VMEM((length, width), bf),
            pltpu.VMEM((length, width), bf),
            pltpu.VMEM((GROUPS * span, width), bf),
            pltpu.VMEM((rows, width), bf),
            sem((3,)),
            sem((COPIES,)),
            sem((COPIES,)),
            sem((KINDS * GROUPS,)),
            sem((KINDS * GROUPS,)),
        ],
        compiler_params=pltpu.CompilerParams(
            collective_id=1, has_side_effects=True, vmem_limit_bytes=63 * 2**20
        ),
    )(*mix_operands(args, residual, norm_gain), *routing, w_gate, w_up, w_down)


def slot_table(routes, capacity, experts):
    flat = routes.reshape(-1)
    count = flat.shape[0]
    onehot = (flat[:, None] == jnp.arange(experts, dtype=jnp.int32)[None, :]).astype(jnp.int32)
    place = jnp.sum((jnp.cumsum(onehot, axis=0) - onehot) * onehot, axis=1)
    table = (
        jnp.full((experts, capacity), count, jnp.int32)
        .at[flat, place]
        .set(jnp.arange(count, dtype=jnp.int32))
    )
    return (table, place)

def body(
    residual,
    query_one,
    key_one,
    value_one,
    gate_one,
    decay_one,
    norm_one,
    output_one,
    query_two,
    key_two,
    value_two,
    gate_two,
    decay_two,
    norm_two,
    output_two,
    norm_gain,
    expert_ids,
    group_weight,
    pair_weight,
    expert_gate,
    expert_up,
    expert_down,
):
    n_sp, n_tp = lax.axis_size("sp"), lax.axis_size("tp")
    mixing = (
        query_one, key_one, value_one, gate_one, decay_one, norm_one, output_one,
        query_two, key_two, value_two, gate_two, decay_two, norm_two, output_two,
    )
    rows_dev = residual.shape[0]
    rank = lax.axis_index("tp")
    experts = n_sp
    capacity = max(2, 2 * rows_dev // (experts - GROUPS) + 1)
    if experts == 2 * GROUPS and n_tp == 4:
        return whole_layer(
            n_sp,
            n_tp,
            mixing,
            residual,
            norm_gain,
            (expert_ids.T, group_weight[None], pair_weight.T),
            capacity,
            expert_gate[0],
            expert_up[0],
            expert_down[0],
        )
    own_routes = lax.dynamic_slice_in_dim(expert_ids, rank * rows_dev, rows_dev, 0)
    own_group = lax.dynamic_slice_in_dim(group_weight, rank * rows_dev, rows_dev, 0)
    own_pair = lax.dynamic_slice_in_dim(pair_weight, rank * rows_dev, rows_dev, 0)
    weights = own_group[:, None] * own_pair / jnp.sum(own_pair, axis=1, keepdims=True)
    stream, normed_rows = mixer(n_sp, n_tp, mixing, residual, norm_gain)
    blank = jnp.zeros((1, D), jnp.bfloat16)
    table, own_place = slot_table(own_routes, capacity, experts)
    index = jnp.where(table == 2 * rows_dev, rows_dev, table // 2)
    send = jnp.concatenate([normed_rows, blank], axis=0)[index][None]
    received = lax.all_to_all(send, "sp", split_axis=1, concat_axis=1, tiled=True)
    received = lax.all_gather(received, "tp", axis=0, tiled=True)
    flat = received.reshape(-1, received.shape[-1])
    gate_part = jnp.dot(flat, expert_gate[0], preferred_element_type=jnp.float32)
    up_part = jnp.dot(flat, expert_up[0], preferred_element_type=jnp.float32)
    hidden = (jax.nn.silu(gate_part) * up_part).astype(jnp.bfloat16)
    share_sum = lax.psum_scatter(
        jnp.dot(hidden, expert_down[0], preferred_element_type=jnp.float32)
        .reshape(received.shape)
        .astype(jnp.bfloat16),
        "tp",
        scatter_dimension=0,
        tiled=True,
    )
    returned = lax.all_to_all(share_sum, "sp", split_axis=1, concat_axis=1, tiled=True)
    slot_index = own_routes.reshape(-1) * capacity + own_place
    picked = returned.reshape(-1, D)[slot_index].astype(jnp.float32).reshape(rows_dev, 2, D)
    layer = stream.astype(jnp.float32) + jnp.sum(weights[:, :, None] * picked, axis=1)
    return layer.astype(jnp.bfloat16)

def solution(mesh):
    placed = (
        P(("sp", "tp"), None),
        P("sp", "tp"),
        P("sp", "tp"),
        P("sp", "tp"),
        P("sp", "tp"),
        P(None, "sp", "tp"),
        P(),
        P("tp", None),
        P("sp", "tp"),
        P("sp", "tp"),
        P("sp", "tp"),
        P("sp", "tp"),
        P(None, "sp", "tp"),
        P(),
        P("tp", None),
        P(),
        P("sp", None),
        P("sp"),
        P("sp", None),
        P("sp", None, "tp"),
        P("sp", None, "tp"),
        P("sp", "tp", None),
    )
    return jax.shard_map(
        body, mesh=mesh, in_specs=placed, out_specs=P(("sp", "tp"), None), check_vma=False
    )
```

```python
import functools

import jax
import jax.numpy as jnp
from jax import lax
from jax.experimental import pallas as pl
from jax.experimental.pallas import tpu as pltpu
from jax.sharding import PartitionSpec as P

D = 2048
KEY_ONE = 64
KEY_TWO = 128
VALUE_W = 128
BLOCK = 64
GROUPS = 4


MESH = pl.DeviceIdType.MESH
TAU = 16.0
EPS = 1e-06


def log_sigmoid(x):
    return jnp.minimum(x, 0.0) - jnp.log1p(jnp.exp(-jnp.abs(x)))


def contract(a, b, dims):
    return lax.dot_general(a, b, (dims, ((), ())), preferred_element_type=jnp.float32)


NN, NT, TN = ((1,), (0,)), ((1,), (1,)), ((0,), (0,))


def flip_bit(index, bit):
    return index + bit - 2 * bit * lax.rem(index // bit, 2)


def meet(peers):
    barrier = pltpu.get_barrier_semaphore()
    for peer in peers:
        pl.semaphore_signal(barrier, inc=1, device_id=peer, device_id_type=MESH)
    pl.semaphore_wait(barrier, len(peers))


def remote(source, target, send, recv, device):
    return pltpu.make_async_remote_copy(
        src_ref=source,
        dst_ref=target,
        send_sem=send,
        recv_sem=recv,
        device_id=device,
        device_id_type=MESH,
    )


def nothing(*_):
    return None


PACK = VALUE_W + 16


def mix(n_sp, n_tp, operands, scratch, ready, sent_states, loaded, got_states, sent_parts):
    q1, k1, v1, g1, d1, q2, k2, v2, g2, d2, norm1, norm2, out1, out2, res, gain = operands
    cum, qd, kd, added, ends, sent, got, carried, total, mixed, part_send, part_got = scratch[:12]
    fade_own, fade_all, half_send, half_got = scratch[12:16]
    st_send, st_recv, pt_send, pt_recv, fd_send, fd_recv, hf_send, hf_recv = scratch[16:]
    sp, tp = lax.axis_index("sp"), lax.axis_index("tp")
    length = q1.shape[0]
    blocks = length // BLOCK
    lanes = 128
    units = []
    for q, k, v, g, d, norm, key in (
        (q1, k1, v1, g1, d1, norm1, KEY_ONE),
        (q2, k2, v2, g2, d2, norm2, KEY_TWO),
    ):
        per = lanes // key
        for at in range(q.shape[1] // lanes):
            units.append((q, k, v, g, d, norm, key, per, at))
    count = len(units)
    bits = [1 << r for r in range(n_tp.bit_length() - 1)]
    paired = n_sp == 2 * GROUPS
    place, side = sp // 2, lax.rem(sp, 2)
    mate = (flip_bit(sp, 1), tp)

    meet(
        [(lax.rem(sp + off, n_sp), tp) for off in range(1, n_sp)]
        + [(sp, flip_bit(tp, bit)) for bit in bits]
        + ready(None)
    )
    ready(True)

    def state_copy(u, off):
        to = lax.rem(sp + off, n_sp)
        way = jnp.where(to > sp, 0, 1)
        rows = slice(u * PACK, (u + 1) * PACK)
        sem = off * count + u
        return remote(
            sent.at[way, rows], got.at[off, rows], st_send.at[sem], st_recv.at[sem], (to, tp)
        )

    def place_copy(u, off):
        z = lax.rem(place + off, GROUPS)
        way = jnp.where(z > place, 0, 1) if off else side
        rows = slice(u * PACK, u * PACK + VALUE_W)
        sem = off * count + u
        return remote(
            sent.at[way, rows],
            got.at[off, rows],
            st_send.at[sem],
            st_recv.at[sem],
            (z * 2 + side, tp) if off else mate,
        )

    def fade_copy(off):
        to = (lax.rem(sp + off, n_sp), tp)
        return remote(fade_own, fade_all.at[off], fd_send.at[off], fd_recv.at[off], to)

    def half_copy(u):
        return remote(half_send.at[u], half_got.at[u], hf_send.at[u], hf_recv.at[u], mate)

    t_at = lax.broadcasted_iota(jnp.int32, (length, length), 0)
    s_at = lax.broadcasted_iota(jnp.int32, (length, length), 1)
    same = (t_at // BLOCK) == (s_at // BLOCK)
    for u, (q, k, v, g, d, norm, key, per, at) in enumerate(units):
        for way in range(2):
            tri = jnp.where(
                same & ((s_at <= t_at) if way == 0 else (s_at >= t_at)), 1.0, 0.0
            ).astype(jnp.bfloat16)
            cols = slice(at * lanes, (at + 1) * lanes)
            rate = log_sigmoid(d[way, :, cols].astype(jnp.float32)) / TAU
            high = rate.astype(jnp.bfloat16)
            rest = rate - high.astype(jnp.float32)
            mid = rest.astype(jnp.bfloat16)
            low = (rest - mid.astype(jnp.float32)).astype(jnp.bfloat16)
            cum[u] = contract(tri, high, NN) + contract(tri, mid, NN) + contract(tri, low, NN)
            state = jnp.zeros((VALUE_W, lanes), jnp.float32)
            reach = jnp.zeros((1, lanes), jnp.float32)
            lane = lax.broadcasted_iota(jnp.int32, (VALUE_W, lanes), 1) // key
            for n in range(blocks) if way == 0 else range(blocks - 1, -1, -1):
                rows = slice(n * BLOCK, (n + 1) * BLOCK)
                c = cum[u, rows, :]
                e = c[BLOCK - 1 : BLOCK] if way == 0 else c[0:1]
                queries = q[rows, cols].astype(jnp.float32) * key ** (-0.5)
                keys = k[rows, cols].astype(jnp.float32)
                qd[way, u, rows, :] = (queries * jnp.exp(c)).astype(jnp.bfloat16)
                kd[way, u, rows, :] = (keys * jnp.exp(-c)).astype(jnp.bfloat16)
                end = (keys * jnp.exp(e - c)).astype(jnp.bfloat16)
                term = None
                for h in range(per):
                    head = at * per + h
                    value = v[rows, head * VALUE_W : (head + 1) * VALUE_W]
                    new = contract(value, end, TN)
                    term = new if term is None else jnp.where(lane == h, new, term)
                added[way, u, n] = term
                fade = jnp.exp(e)
                ends[way, u, n : n + 1, :] = fade
                state = state * fade + term
                reach = reach + e
            sent[way, u * PACK : u * PACK + VALUE_W, :] = state.astype(jnp.bfloat16)
            if paired:
                row = way * count + u
                fade_own[row : row + 1, :] = jnp.exp(reach)
            else:
                sent[way, u * PACK + VALUE_W : (u + 1) * PACK, :] = jnp.broadcast_to(
                    jnp.exp(reach), (16, lanes)
                ).astype(jnp.bfloat16)

        if paired:
            for off in (1, 2, 3, 0):
                place_copy(u, off).start()
        else:

            @pl.loop(1, n_sp)
            def _(off):
                state_copy(u, off).start()

    if paired:

        @pl.loop(1, n_sp)
        def _(off):
            fade_copy(off).start()

    sent_states()
    t_blk = lax.broadcasted_iota(jnp.int32, (BLOCK, BLOCK), 0)
    s_blk = lax.broadcasted_iota(jnp.int32, (BLOCK, BLOCK), 1)
    first = 0
    for u, (q, k, v, g, d, norm, key, per, at) in enumerate(units):
        lane = lax.broadcasted_iota(jnp.int32, (BLOCK, lanes), 1) // key
        for h in range(per):
            head = at * per + h
            for n in range(blocks):
                rows = slice(n * BLOCK, (n + 1) * BLOCK)
                scores = None
                for way in range(2):
                    queries = qd[way, u, rows, :]
                    if per > 1:
                        queries = jnp.where(lane == h, queries, jnp.zeros_like(queries))
                    one = contract(queries, kd[way, u, rows, :], NT)
                    one = jnp.where((s_blk <= t_blk) if way == 0 else (s_blk >= t_blk), one, 0.0)
                    scores = one if scores is None else scores + one
                value = v[rows, head * VALUE_W : (head + 1) * VALUE_W]
                total[first + h, rows, :] = contract(scores.astype(jnp.bfloat16), value, NN)
        first += per

    carried[...] = jnp.zeros_like(carried)

    def fold(way, who):
        off = lax.rem(sp - who + n_sp, n_sp)
        for u in range(count):
            fade = got[off, u * PACK + VALUE_W : (u + 1) * PACK, :][0:1]
            state = got[off, u * PACK : u * PACK + VALUE_W, :]
            carried[way, u] = carried[way, u] * fade.astype(jnp.float32) + state.astype(jnp.float32)

    def fade_of(who, way, u):
        row = way * count + u
        return fade_all[lax.rem(sp - who + n_sp, n_sp), row : row + 1, :]

    def fold_place(way, u, z):
        off = lax.rem(place - z + GROUPS, GROUPS)
        fades = [fade_of(2 * z + y, way, u) for y in range(2)]
        state = got[off, u * PACK : u * PACK + VALUE_W, :].astype(jnp.float32)
        later = jnp.where(side == way, fades[1 - way], jnp.ones_like(fades[0]))
        carried[way, u] = carried[way, u] * (fades[0] * fades[1]) + state * later

    if paired:

        @pl.loop(1, n_sp)
        def _(off):
            fade_copy(off).wait()

        for u in range(count):
            for off in range(1, GROUPS):
                place_copy(u, off).wait()

            @pl.loop(0, place)
            def _(z):
                fold_place(0, u, z)

            @pl.loop(0, GROUPS - 1 - place)
            def _(back):
                fold_place(1, u, GROUPS - 1 - back)

            half_send[u] = carried[:, u].astype(jnp.bfloat16)
            half_copy(u).start()
        got_states()
        loaded()
        for u in range(count):
            place_copy(u, 0).wait()
            half_copy(u).wait()
            carried[:, u] = carried[:, u] + half_got[u].astype(jnp.float32)
            way = 1 - side
            off = 1 + way * (n_sp - 2)
            fade = fade_all[off, pl.ds(way * count + u, 1), :]
            state = got[0, u * PACK : u * PACK + VALUE_W, :].astype(jnp.float32)
            carried[way, u] = carried[way, u] * fade + state
    else:

        @pl.loop(1, n_sp)
        def _(off):
            for u in range(count):
                state_copy(u, off).wait()

        @pl.loop(0, sp)
        def _(who):
            fold(0, who)

        @pl.loop(0, n_sp - 1 - sp)
        def _(back):
            fold(1, n_sp - 1 - back)

    first = 0
    for u, (q, k, v, g, d, norm, key, per, at) in enumerate(units):
        lane = lax.broadcasted_iota(jnp.int32, (BLOCK, lanes), 1) // key
        for way in range(2):
            state = carried[way, u]
            for n in range(blocks) if way == 0 else range(blocks - 1, -1, -1):
                rows = slice(n * BLOCK, (n + 1) * BLOCK)
                low = state.astype(jnp.bfloat16)
                for h in range(per):
                    queries = qd[way, u, rows, :]
                    if per > 1:
                        queries = jnp.where(lane == h, queries, jnp.zeros_like(queries))
                    total[first + h, rows, :] += contract(queries, low, NT)
                state = state * ends[way, u, n : n + 1, :] + added[way, u, n]
        for h in range(per):
            head = at * per + h
            cols = slice(head * VALUE_W, (head + 1) * VALUE_W)
            x = total[first + h]
            y = x * lax.rsqrt(jnp.mean(x * x, axis=-1, keepdims=True) + EPS) * norm[...]
            gate = g[:, cols].astype(jnp.float32)
            y = y * (gate / (1.0 + jnp.exp(-gate)))
            mixed[:, (first + h) * VALUE_W : (first + h + 1) * VALUE_W] = y.astype(jnp.bfloat16)
        first += per

    rows_dev = res.shape[0]
    split = out1.shape[0]

    def project(mask):
        block = tp
        for bit in bits:
            if mask & bit:
                block = flip_bit(block, bit)
        rows = pl.ds(pl.multiple_of(block * rows_dev, 16), rows_dev)
        return contract(mixed[rows, :split], out1[...], NN) + contract(
            mixed[rows, split:], out2[...], NN
        )

    def part_copy(mask, bit):
        return remote(
            part_send.at[mask],
            part_got.at[mask],
            pt_send.at[mask],
            pt_recv.at[mask],
            (sp, flip_bit(tp, bit)),
        )

    low_bit = lambda m: m & -m
    order = sorted(range(1, n_tp), key=lambda m: (low_bit(m), -m))
    for mask in order:
        bit = low_bit(mask)
        value = project(mask)
        for earlier in bits:
            if earlier < bit:
                part_copy(mask | earlier, earlier).wait_recv()
                value = value + part_got[mask | earlier].astype(jnp.float32)
        part_send[mask] = value.astype(jnp.bfloat16)
        part_copy(mask, bit).start()
    sent_parts()
    value = project(0)
    for bit in bits:
        part_copy(bit, bit).wait_recv()
        value = value + part_got[bit].astype(jnp.float32)
    stream = (res[...].astype(jnp.float32) + value.astype(jnp.bfloat16).astype(jnp.float32)).astype(
        jnp.bfloat16
    )
    wide = stream.astype(jnp.float32)
    scale = lax.rsqrt(jnp.mean(wide * wide, axis=-1, keepdims=True) + EPS)
    normed = (wide * scale * gain[...]).astype(jnp.bfloat16)
    return stream, normed, [part_copy(mask, low_bit(mask)) for mask in order]


def mix_scratch(n_sp, n_tp, args, residual):
    q1, k1, v1, g1, d1, norm1, out1, q2, k2, v2, g2, d2, norm2, out2 = args
    length = q1.shape[0]
    blocks = length // BLOCK
    count = (q1.shape[1] + q2.shape[1]) // 128
    heads = (v1.shape[1] + v2.shape[1]) // VALUE_W
    rows, width = residual.shape
    packed = count * PACK
    bf, f32 = jnp.bfloat16, jnp.float32
    sem = pltpu.SemaphoreType.DMA
    return [
        pltpu.VMEM((count, length, 128), f32),
        pltpu.VMEM((2, count, length, 128), bf),
        pltpu.VMEM((2, count, length, 128), bf),
        pltpu.VMEM((2, count, blocks, VALUE_W, 128), f32),
        pltpu.VMEM((2, count, -(-blocks // 8) * 8, 128), f32),
        pltpu.VMEM((2, packed, 128), bf),
        pltpu.VMEM((n_sp, packed, 128), bf),
        pltpu.VMEM((2, count, VALUE_W, 128), f32),
        pltpu.VMEM((heads, length, VALUE_W), f32),
        pltpu.VMEM((length, heads * VALUE_W), bf),
        pltpu.VMEM((n_tp, rows, width), bf),
        pltpu.VMEM((n_tp, rows, width), bf),
        pltpu.VMEM((-(-2 * count // 8) * 8, 128), f32),
        pltpu.VMEM((n_sp, -(-2 * count // 8) * 8, 128), f32),
        pltpu.VMEM((count, 2, VALUE_W, 128), bf),
        pltpu.VMEM((count, 2, VALUE_W, 128), bf),
        sem((n_sp * count,)),
        sem((n_sp * count,)),
        sem((n_tp,)),
        sem((n_tp,)),
        sem((n_sp,)),
        sem((n_sp,)),
        sem((count,)),
        sem((count,)),
    ]


def mix_operands(args, residual, norm_gain):
    q1, k1, v1, g1, d1, norm1, out1, q2, k2, v2, g2, d2, norm2, out2 = args
    return (
        q1, k1, v1, g1, d1, q2, k2, v2, g2, d2,
        norm1[None], norm2[None], out1, out2, residual, norm_gain[None],
    )


def mixer_kernel(n_sp, n_tp, *refs):
    operands, (stream_ref, normed_ref), scratch = refs[:16], refs[16:18], refs[18:]
    ready = lambda go: [] if go is None else None
    stream, normed, pending = mix(
        n_sp, n_tp, operands, scratch, ready, nothing, nothing, nothing, nothing
    )
    stream_ref[...] = stream
    normed_ref[...] = normed
    for one in pending:
        one.wait_send()


def mixer(n_sp, n_tp, args, residual, norm_gain):
    rows, width = residual.shape
    vmem = pl.BlockSpec(memory_space=pltpu.VMEM)
    return pl.pallas_call(
        functools.partial(mixer_kernel, n_sp, n_tp),
        out_shape=(jax.ShapeDtypeStruct((rows, width), jnp.bfloat16),) * 2,
        in_specs=[vmem] * 16,
        out_specs=(vmem, vmem),
        scratch_shapes=mix_scratch(n_sp, n_tp, args, residual),
        compiler_params=pltpu.CompilerParams(
            collective_id=0, has_side_effects=True, vmem_limit_bytes=60 * 2**20
        ),
    )(*mix_operands(args, residual, norm_gain))


ORDER = ((0, 1, 2, 3), (1, 3, 2, 0))
SEND = ((0, 2, 1, 3), (1, 0, 3, 2))


def mirror(place):
    turned, last = place // (GROUPS // 2), GROUPS - 1
    return turned, place + turned * (last - 2 * place)


def place_at(place, rank, table):
    turned, inner = mirror(place)
    end, mid = table[0][rank], table[1][rank]
    spot = end + inner * (mid - end)
    return spot + turned * (GROUPS - 1 - 2 * spot)


def rank_in(place, other, table):
    turned, inner = mirror(place)
    spot = other + turned * (GROUPS - 1 - 2 * other)
    end, mid = (
        sum(jnp.where(spot == row[rank], rank, 0) for rank in range(GROUPS)) for row in table
    )
    return end + inner * (mid - end)


KINDS = 5
COPIES = 10 * GROUPS + 4 * GROUPS + 8


def layer_kernel(n_sp, n_tp, stride, over, extra, n_scratch, *refs):
    given = refs[:16]
    ids, group_share, pair_share, w_gate, w_up, w_down, out_ref = refs[16:23]
    scratch = refs[23 : 23 + n_scratch]
    operands = refs[23 + n_scratch : 39 + n_scratch]
    (
        v_gate, v_up, wd, spread, meta_send, meta_got, wslot, z_send, z_extra, data, hid, hgot,
        acc, part, pgot, outs, back_got, kept, w_sem, o_sem, s_sem, r_sem, zs_sem, zr_sem,
    ) = refs[39 + n_scratch :]
    bf, f32 = jnp.bfloat16, jnp.float32
    sp, tp = lax.axis_index("sp"), lax.axis_index("tp")
    span = stride + extra
    length = GROUPS * stride + extra
    wire = -(-GROUPS * over // 8) * 8
    width = data.shape[2]
    units = hid.shape[2]
    place, side = sp // 2, lax.rem(sp, 2)
    core, across, along = (sp, flip_bit(tp, 1)), (sp, flip_bit(tp, 2)), (flip_bit(sp, 1), tp)
    corner = (flip_bit(sp, 1), flip_bit(tp, 2))
    cut = width // 256 * 128
    left, right = slice(0, cut), slice(cut, width)
    far, home = [], []
    for i in range(1, GROUPS):
        z = place_at(place, i, SEND)
        far.append((i, rank_in(z, place, ORDER), (z * 2 + side, tp)))
        z = place_at(place, i, ORDER)
        home.append((i, rank_in(z, place, SEND), (z * 2 + side, tp)))
    numbers = iter(range(COPIES))
    started = []

    def copy(source, target, device):
        number = next(numbers)
        return remote(source, target, s_sem.at[number], r_sem.at[number], device)

    def go(one):
        one.start()
        started.append(one)
        return one

    def z_copy(kind, i, rank, source, target, device):
        return remote(
            source,
            target,
            zs_sem.at[kind * GROUPS + i],
            zr_sem.at[kind * GROUPS + rank],
            device,
        )

    loads = [
        pltpu.make_async_copy(source, target, w_sem.at[i])
        for i, (source, target) in enumerate(
            ((w_gate, v_gate), (w_up, v_up), (w_down, wd.at[0]))
        )
    ]
    late = (3, 8, 10, 11, 12, 13, 14, 15)
    moves = [
        pltpu.make_async_copy(given[i], operands[i], o_sem.at[i]) for i in range(len(operands))
    ]
    quarter = units // 4
    down_y = [
        copy(w_down.at[rows], wd.at[1, rows], along)
        for rows in (
            slice(0, quarter), slice(quarter, 3 * quarter), slice(3 * quarter, units)
        )
    ]
    down_x = copy(w_down, wd.at[2], across)
    upper, middle = slice(0, quarter), slice(quarter, 2 * quarter)
    lower = slice(2 * quarter, units)
    down_yx = [copy(wd.at[1, rows], wd.at[3, rows], across) for rows in (upper, middle)]
    down_xy = copy(wd.at[2, lower], wd.at[3, lower], along)
    metas = [
        z_copy(4, i, rank, meta_send.at[slice(i * span, (i + 1) * span)], meta_got.at[rank], to)
        for i, rank, to in far
    ]
    meta_core = copy(wslot.at[0], wslot.at[1], core)

    def block(index):
        return slice(index * span, (index + 1) * span)

    def chunk(o):
        return slice(o * stride, (o + 1) * stride if o < GROUPS - 1 else length)

    def moved(o):
        return slice(o * stride, (o + 1) * stride if o < GROUPS - 1 else GROUPS * stride + wire)

    def routing():
        rows, tokens = spread.shape[1], ids.shape[1]
        first, share = ids[0:1, :], group_share[...]
        kind = lax.broadcasted_iota(jnp.int32, (8, 1), 0)
        member = ((first >= 2 * kind) & (first < 2 * kind + 2)).astype(f32)
        from_at = lax.broadcasted_iota(jnp.int32, (tokens, tokens), 0)
        to_at = lax.broadcasted_iota(jnp.int32, (tokens, tokens), 1)
        before = jnp.where((from_at < to_at) & (from_at // rows == to_at // rows), 1.0, 0.0)
        counts = contract(member.astype(bf), before.astype(bf), NN)
        nth = jnp.sum(member * counts, axis=0, keepdims=True)
        named = lax.rem(kind, GROUPS)
        base = (rank_in(place, named, SEND) * span).astype(f32)
        shift = (rank_in(named, place, ORDER) * over).astype(f32)
        seat = base + jnp.where(nth < stride, nth, nth + shift)
        seat = jnp.sum(member * seat, axis=0, keepdims=True)
        pair = pair_share[0:1, :] + pair_share[1:2, :]
        w_first = share * pair_share[0:1, :] / pair
        w_second = share * pair_share[1:2, :] / pair
        even = lax.rem(first, 2) == 0
        table = jnp.zeros((8, tokens), f32)
        table = jnp.where(kind == 0, seat, table)
        for s in range(2):
            w = jnp.where(even, w_first, w_second) if s == 0 else jnp.where(even, w_second, w_first)
            high = w.astype(bf).astype(f32)
            table = jnp.where(kind == 1 + s, high, table)
            table = jnp.where(kind == 3 + s, w - high, table)
        at = lax.broadcasted_iota(jnp.int32, (tokens, rows), 0)
        own_at = lax.broadcasted_iota(jnp.int32, (tokens, rows), 1) + tp * rows
        select = jnp.where(at == own_at, 1.0, 0.0).astype(bf)
        table = contract(table.astype(bf), select, NN)
        seats = lax.broadcasted_iota(jnp.int32, (GROUPS * span, rows), 0)
        spread[...] = jnp.where(seats == table[0:1].astype(jnp.int32), 1.0, 0.0).astype(bf)
        line = lax.broadcasted_iota(jnp.int32, (128, 1), 0)
        lines = jnp.zeros((128, rows), f32)
        for row, spot in ((1, 0), (2, 1), (3, 64), (4, 65)):
            lines = jnp.where(line == spot, table[row : row + 1], lines)
        meta_send[...] = contract(spread[...], lines.astype(bf), NT).astype(bf)

    def ready(begin):
        if begin is None:
            return [corner]
        go(down_x)
        go(down_y[0])
        for load in loads:
            load.start()
        for i, move in enumerate(moves):
            if i not in late:
                move.wait()

    def sent_states():
        go(down_y[1])
        routing()
        for one in metas:
            go(one)
        rest = slice(GROUPS * stride + wire, length)
        if wire < extra:
            data[:, rest, :] = jnp.zeros((8, extra - wire, width), bf)
            hgot[:, :, rest, :] = jnp.zeros((3, 2, extra - wire, units), bf)
            pgot[rest, :] = jnp.zeros((extra - wire, width), bf)
            for i in range(GROUPS):
                spare = slice(i * span + stride + wire, (i + 1) * span)
                back_got[spare, :] = jnp.zeros((extra - wire, width), bf)
    def loaded():
        for i in late:
            moves[i].wait()

    def sent_parts():
        down_y[1].wait_recv()
        go(down_yx[1])
        down_x.wait_recv()
        go(down_xy)

    def meta_wait(o):
        z_copy(4, 0, o, meta_send.at[block(o)], meta_got.at[o], core).wait_recv()

    def got_states():
        own = meta_send[block(0)]
        wslot[0, 0:stride] = own[:stride]
        more = own[stride:].astype(f32)
        for o in range(1, GROUPS):
            meta_wait(o)
            wslot[0, o * stride : (o + 1) * stride] = meta_got[o, :stride]
            more = more + meta_got[o, stride:].astype(f32)
        wslot[0, GROUPS * stride :] = more.astype(bf)
        go(meta_core)
        down_y[0].wait_recv()
        go(down_yx[0])
        go(down_y[2])

    for i in sorted(range(len(moves)), key=lambda i: i in late):
        moves[i].start()
    stream, normed, pending = mix(
        n_sp, n_tp, operands, scratch, ready, sent_states, loaded, got_states, sent_parts
    )
    kept[...] = stream

    for i, rank, to in far:
        z_send[block(i)] = contract(spread[block(i), :], normed, NN).astype(bf)
        go(
            z_copy(
                0, i, rank,
                z_send.at[slice(i * span, i * span + stride)],
                data.at[0, pl.ds(pl.multiple_of(rank * stride, 16), stride)],
                to,
            )
        )
        go(
            z_copy(
                1, i, rank,
                z_send.at[slice(i * span + stride, i * span + stride + wire)],
                z_extra.at[rank],
                to,
            )
        )
    own = contract(spread[block(0), :], normed, NN).astype(bf)
    data[0, chunk(0), :] = own[:stride]
    z_extra[0] = own[stride : stride + wire]

    flows = []
    for o in range(GROUPS):
        ch = moved(o)
        flows.append(
            dict(
                a_y=copy(data.at[0, ch, left], data.at[2, ch, left], along),
                b_x=copy(data.at[0, ch, right], data.at[4, ch, right], across),
                a_x=copy(data.at[0, ch, left], data.at[4, ch, left], across),
                b_y=copy(data.at[0, ch, right], data.at[2, ch, right], along),
                c_0=copy(data.at[0, ch], data.at[1, ch], core),
                a_d=copy(data.at[2, ch, left], data.at[6, ch, left], across),
                b_d=copy(data.at[4, ch, right], data.at[6, ch, right], along),
                c_y=copy(data.at[2, ch], data.at[3, ch], core),
                c_x=copy(data.at[4, ch], data.at[5, ch], core),
                c_d=copy(data.at[6, ch], data.at[7, ch], core),
                h_y=copy(hid.at[slice(2, 4), ch], hgot.at[0, :, ch], along),
                h_x=copy(hid.at[slice(4, 6), ch], hgot.at[1, :, ch], across),
                h_d=copy(hid.at[slice(6, 8), ch], hgot.at[2, :, ch], corner),
                p_c=copy(part.at[ch], pgot.at[ch], core),
            )
        )

    def arrive(kind, o, target):
        z_copy(kind, 0, o, target, target, core).wait_recv()

    def stage(o):
        flow = flows[o]
        if o:
            arrive(0, o, data.at[0, slice(o * stride, (o + 1) * stride)])
        if o == GROUPS - 1:
            more = z_extra[0].astype(f32)
            for k in range(1, GROUPS):
                arrive(1, k, z_extra.at[k])
                more = more + z_extra[k].astype(f32)
            data[0, GROUPS * stride : GROUPS * stride + wire, :] = more.astype(bf)
        for name in ("a_y", "b_x", "a_x", "b_y", "c_0"):
            go(flow[name])

    def forward(o):
        flow = flows[o]
        flow["a_y"].wait_recv()
        go(flow["a_d"])
        flow["b_x"].wait_recv()
        go(flow["b_d"])
        flow["b_y"].wait_recv()
        go(flow["c_y"])
        flow["a_x"].wait_recv()
        go(flow["c_x"])

    def finish(o):
        flow = flows[o]
        flow["a_d"].wait_recv()
        flow["b_d"].wait_recv()
        go(flow["c_d"])

    def compute(o):
        flow, ch = flows[o], chunk(o)
        for name in ("c_0", "c_y", "c_x", "c_d"):
            flow[name].wait_recv()
        n = ch.stop - ch.start

        @pl.loop(0, 2)
        def _(m):
            some = pl.ds(m * 4, 4)
            x = data[some, ch, :].reshape(4 * n, width)
            gate = contract(x, v_gate[...], NN)
            up = contract(x, v_up[...], NN)
            hidden = (gate / (1.0 + jnp.exp(-gate)) * up).astype(bf)
            hid[some, ch, :] = hidden.reshape(4, n, units)

        for name in ("h_y", "h_x", "h_d"):
            go(flow[name])

    lane = lax.broadcasted_iota(jnp.int32, (1, 128), 1)

    def down(o):
        flow, ch = flows[o], chunk(o)
        n = ch.stop - ch.start
        w = wslot[:, ch, :].reshape(2 * n, 128).astype(f32)
        pick = lambda s: jnp.sum(
            jnp.where((lane == s) | (lane == s + 64), w, 0.0), axis=1, keepdims=True
        )
        mine, other = pick(side), pick(1 - side)
        for name in ("h_y", "h_x", "h_d"):
            flow[name].wait_recv()
        tile = 512

        @pl.loop(0, width // tile)
        def _(j):
            cols = pl.ds(pl.multiple_of(j * tile, tile), tile)
            rows = lambda value: value.reshape(2 * n, units)
            a = contract(rows(hid[0:2, ch, :]), wd[0, :, cols], NN) + contract(
                rows(hgot[1, :, ch, :]), wd[2, :, cols], NN
            )
            b = contract(rows(hgot[0, :, ch, :]), wd[1, :, cols], NN) + contract(
                rows(hgot[2, :, ch, :]), wd[3, :, cols], NN
            )
            value = a * mine + b * other
            acc[ch, cols] = value[:n]
            part[ch, cols] = value[n:].astype(bf)

        go(flow["p_c"])

    def give(o):
        flow, ch = flows[o], chunk(o)
        flow["p_c"].wait_recv()
        outs[ch, :] = (acc[ch, :] + pgot[ch, :].astype(f32)).astype(bf)
        rows = slice(o * stride, (o + 1) * stride)
        if o == 0:
            back_got[0:stride] = outs[rows, :]
        else:
            i, rank, to = home[o - 1]
            go(
                z_copy(
                    2, i, rank,
                    outs.at[rows],
                    back_got.at[pl.ds(pl.multiple_of(rank * span, 16), stride)],
                    to,
                )
            )
        if o == GROUPS - 1:
            rows = slice(GROUPS * stride, GROUPS * stride + wire)
            back_got[stride : stride + wire] = outs[rows, :]
            for i, rank, to in home:
                go(
                    z_copy(
                        3, i, rank,
                        outs.at[rows],
                        back_got.at[pl.ds(pl.multiple_of(rank * span + stride, 16), wire)],
                        to,
                    )
                )

    stage(0)
    forward(0)
    for load in loads:
        load.wait()
    finish(0)
    compute(0)
    stage(1)
    forward(1)
    stage(2)
    finish(1)
    compute(1)
    forward(2)
    stage(3)
    meta_core.wait_recv()
    for one in (down_y[2], *down_yx, down_xy):
        one.wait_recv()
    down(0)
    down(1)
    finish(2)
    compute(2)
    give(1)
    forward(3)
    down(2)
    finish(3)
    compute(3)
    give(2)
    give(0)
    down(3)
    give(3)
    for i in range(1, GROUPS):
        arrive(2, i, back_got.at[slice(i * span, i * span + stride)])
        arrive(3, i, back_got.at[slice(i * span + stride, i * span + stride + wire)])
    picked = contract(spread[...], back_got[...], TN)
    out_ref[...] = (kept[...].astype(f32) + picked).astype(bf)
    for one in pending + started:
        one.wait_send()


def whole_layer(n_sp, n_tp, args, residual, norm_gain, routing, capacity, w_gate, w_up, w_down):
    rows, width = residual.shape
    units = w_gate.shape[1]
    stride = capacity // 16 * 16
    over = capacity - stride
    extra = max(16, -(-GROUPS * over // 16) * 16)
    span, length = stride + extra, GROUPS * stride + extra
    bf, f32 = jnp.bfloat16, jnp.float32
    vmem = pl.BlockSpec(memory_space=pltpu.VMEM)
    hbm = pl.BlockSpec(memory_space=pl.ANY)
    sem = pltpu.SemaphoreType.DMA
    mine = mix_scratch(n_sp, n_tp, args, residual)
    given = mix_operands(args, residual, norm_gain)
    return pl.pallas_call(
        functools.partial(layer_kernel, n_sp, n_tp, stride, over, extra, len(mine)),
        out_shape=jax.ShapeDtypeStruct((rows, width), bf),
        in_specs=[hbm] * 16 + [vmem] * 3 + [hbm] * 3,
        out_specs=vmem,
        scratch_shapes=mine
        + [pltpu.VMEM(one.shape, one.dtype) for one in given]
        + [
            pltpu.VMEM(w_gate.shape, bf),
            pltpu.VMEM(w_up.shape, bf),
            pltpu.VMEM((4, units, width), bf),
            pltpu.VMEM((GROUPS * span, rows), bf),
            pltpu.VMEM((GROUPS * span, 128), bf),
            pltpu.VMEM((GROUPS, span, 128), bf),
            pltpu.VMEM((2, length, 128), bf),
            pltpu.VMEM((GROUPS * span, width), bf),
            pltpu.VMEM((GROUPS, -(-GROUPS * over // 8) * 8, width), bf),
            pltpu.VMEM((8, length, width), bf),
            pltpu.VMEM((8, length, units), bf),
            pltpu.VMEM((3, 2, length, units), bf),
            pltpu.VMEM((length, width), f32),
            pltpu.VMEM((length, width), bf),
            pltpu.VMEM((length, width), bf),
            pltpu.VMEM((length, width), bf),
            pltpu.VMEM((GROUPS * span, width), bf),
            pltpu.VMEM((rows, width), bf),
            sem((3,)),
            sem((16,)),
            sem((COPIES,)),
            sem((COPIES,)),
            sem((KINDS * GROUPS,)),
            sem((KINDS * GROUPS,)),
        ],
        compiler_params=pltpu.CompilerParams(
            collective_id=1, has_side_effects=True, vmem_limit_bytes=63 * 2**20
        ),
    )(*given, *routing, w_gate, w_up, w_down)


def slot_table(routes, capacity, experts):
    flat = routes.reshape(-1)
    count = flat.shape[0]
    onehot = (flat[:, None] == jnp.arange(experts, dtype=jnp.int32)[None, :]).astype(jnp.int32)
    place = jnp.sum((jnp.cumsum(onehot, axis=0) - onehot) * onehot, axis=1)
    table = (
        jnp.full((experts, capacity), count, jnp.int32)
        .at[flat, place]
        .set(jnp.arange(count, dtype=jnp.int32))
    )
    return (table, place)

def body(
    residual,
    query_one,
    key_one,
    value_one,
    gate_one,
    decay_one,
    norm_one,
    output_one,
    query_two,
    key_two,
    value_two,
    gate_two,
    decay_two,
    norm_two,
    output_two,
    norm_gain,
    expert_ids,
    group_weight,
    pair_weight,
    expert_gate,
    expert_up,
    expert_down,
):
    n_sp, n_tp = lax.axis_size("sp"), lax.axis_size("tp")
    mixing = (
        query_one, key_one, value_one, gate_one, decay_one, norm_one, output_one,
        query_two, key_two, value_two, gate_two, decay_two, norm_two, output_two,
    )
    rows_dev = residual.shape[0]
    rank = lax.axis_index("tp")
    experts = n_sp
    capacity = max(2, 2 * rows_dev // (experts - GROUPS) + 1)
    if experts == 2 * GROUPS and n_tp == 4:
        return whole_layer(
            n_sp,
            n_tp,
            mixing,
            residual,
            norm_gain,
            (expert_ids.T, group_weight[None], pair_weight.T),
            capacity,
            expert_gate[0],
            expert_up[0],
            expert_down[0],
        )
    own_routes = lax.dynamic_slice_in_dim(expert_ids, rank * rows_dev, rows_dev, 0)
    own_group = lax.dynamic_slice_in_dim(group_weight, rank * rows_dev, rows_dev, 0)
    own_pair = lax.dynamic_slice_in_dim(pair_weight, rank * rows_dev, rows_dev, 0)
    weights = own_group[:, None] * own_pair / jnp.sum(own_pair, axis=1, keepdims=True)
    stream, normed_rows = mixer(n_sp, n_tp, mixing, residual, norm_gain)
    blank = jnp.zeros((1, D), jnp.bfloat16)
    table, own_place = slot_table(own_routes, capacity, experts)
    index = jnp.where(table == 2 * rows_dev, rows_dev, table // 2)
    send = jnp.concatenate([normed_rows, blank], axis=0)[index][None]
    received = lax.all_to_all(send, "sp", split_axis=1, concat_axis=1, tiled=True)
    received = lax.all_gather(received, "tp", axis=0, tiled=True)
    flat = received.reshape(-1, received.shape[-1])
    gate_part = jnp.dot(flat, expert_gate[0], preferred_element_type=jnp.float32)
    up_part = jnp.dot(flat, expert_up[0], preferred_element_type=jnp.float32)
    hidden = (jax.nn.silu(gate_part) * up_part).astype(jnp.bfloat16)
    share_sum = lax.psum_scatter(
        jnp.dot(hidden, expert_down[0], preferred_element_type=jnp.float32)
        .reshape(received.shape)
        .astype(jnp.bfloat16),
        "tp",
        scatter_dimension=0,
        tiled=True,
    )
    returned = lax.all_to_all(share_sum, "sp", split_axis=1, concat_axis=1, tiled=True)
    slot_index = own_routes.reshape(-1) * capacity + own_place
    picked = returned.reshape(-1, D)[slot_index].astype(jnp.float32).reshape(rows_dev, 2, D)
    layer = stream.astype(jnp.float32) + jnp.sum(weights[:, :, None] * picked, axis=1)
    return layer.astype(jnp.bfloat16)

def solution(mesh):
    placed = (
        P(("sp", "tp"), None),
        P("sp", "tp"),
        P("sp", "tp"),
        P("sp", "tp"),
        P("sp", "tp"),
        P(None, "sp", "tp"),
        P(),
        P("tp", None),
        P("sp", "tp"),
        P("sp", "tp"),
        P("sp", "tp"),
        P("sp", "tp"),
        P(None, "sp", "tp"),
        P(),
        P("tp", None),
        P(),
        P("sp", None),
        P("sp"),
        P("sp", None),
        P("sp", None, "tp"),
        P("sp", None, "tp"),
        P("sp", "tp", None),
    )
    return jax.shard_map(
        body, mesh=mesh, in_specs=placed, out_specs=P(("sp", "tp"), None), check_vma=False
    )
```

```python
import functools

import jax
import jax.numpy as jnp
from jax import lax
from jax.experimental import pallas as pl
from jax.experimental.pallas import tpu as pltpu
from jax.sharding import PartitionSpec as P

D = 2048
KEY_ONE = 64
KEY_TWO = 128
VALUE_W = 128
BLOCK = 64
GROUPS = 4


MESH = pl.DeviceIdType.MESH
TAU = 16.0
EPS = 1e-06


def log_sigmoid(x):
    return jnp.minimum(x, 0.0) - jnp.log1p(jnp.exp(-jnp.abs(x)))


def contract(a, b, dims):
    return lax.dot_general(a, b, (dims, ((), ())), preferred_element_type=jnp.float32)


NN, NT, TN = ((1,), (0,)), ((1,), (1,)), ((0,), (0,))


def flip_bit(index, bit):
    return index + bit - 2 * bit * lax.rem(index // bit, 2)


def meet(peers):
    barrier = pltpu.get_barrier_semaphore()
    for peer in peers:
        pl.semaphore_signal(barrier, inc=1, device_id=peer, device_id_type=MESH)
    pl.semaphore_wait(barrier, len(peers))


def remote(source, target, send, recv, device):
    return pltpu.make_async_remote_copy(
        src_ref=source,
        dst_ref=target,
        send_sem=send,
        recv_sem=recv,
        device_id=device,
        device_id_type=MESH,
    )


def nothing(*_):
    return None


PACK = VALUE_W + 16


def mix(n_sp, n_tp, operands, scratch, ready, sent_states, loaded, got_states, sent_parts):
    q1, k1, v1, g1, d1, q2, k2, v2, g2, d2, norm1, norm2, out1, out2, res, gain = operands
    cum, qd, kd, added, ends, sent, got, carried, total, mixed, part_send, part_got = scratch[:12]
    fade_own, fade_all, half_send, half_got = scratch[12:16]
    st_send, st_recv, pt_send, pt_recv, fd_send, fd_recv, hf_send, hf_recv = scratch[16:]
    sp, tp = lax.axis_index("sp"), lax.axis_index("tp")
    length = q1.shape[0]
    blocks = length // BLOCK
    lanes = 128
    units = []
    for q, k, v, g, d, norm, key in (
        (q1, k1, v1, g1, d1, norm1, KEY_ONE),
        (q2, k2, v2, g2, d2, norm2, KEY_TWO),
    ):
        per = lanes // key
        for at in range(q.shape[1] // lanes):
            units.append((q, k, v, g, d, norm, key, per, at))
    count = len(units)
    bits = [1 << r for r in range(n_tp.bit_length() - 1)]
    paired = n_sp == 2 * GROUPS
    place, side = sp // 2, lax.rem(sp, 2)
    mate = (flip_bit(sp, 1), tp)

    meet(
        [(lax.rem(sp + off, n_sp), tp) for off in range(1, n_sp)]
        + [(sp, flip_bit(tp, bit)) for bit in bits]
        + ready(None)
    )
    ready(True)

    def state_copy(u, off):
        to = lax.rem(sp + off, n_sp)
        way = jnp.where(to > sp, 0, 1)
        rows = slice(u * PACK, (u + 1) * PACK)
        sem = off * count + u
        return remote(
            sent.at[way, rows], got.at[off, rows], st_send.at[sem], st_recv.at[sem], (to, tp)
        )

    def place_copy(u, off):
        z = lax.rem(place + off, GROUPS)
        way = jnp.where(z > place, 0, 1) if off else side
        rows = slice(u * PACK, u * PACK + VALUE_W)
        sem = off * count + u
        return remote(
            sent.at[way, rows],
            got.at[off, rows],
            st_send.at[sem],
            st_recv.at[sem],
            (z * 2 + side, tp) if off else mate,
        )

    def fade_copy(off):
        to = (lax.rem(sp + off, n_sp), tp)
        return remote(fade_own, fade_all.at[off], fd_send.at[off], fd_recv.at[off], to)

    def half_copy(u):
        return remote(half_send.at[u], half_got.at[u], hf_send.at[u], hf_recv.at[u], mate)

    t_at = lax.broadcasted_iota(jnp.int32, (length, length), 0)
    s_at = lax.broadcasted_iota(jnp.int32, (length, length), 1)
    same = (t_at // BLOCK) == (s_at // BLOCK)
    for u, (q, k, v, g, d, norm, key, per, at) in enumerate(units):
        for way in range(2):
            tri = jnp.where(
                same & ((s_at <= t_at) if way == 0 else (s_at >= t_at)), 1.0, 0.0
            ).astype(jnp.bfloat16)
            cols = slice(at * lanes, (at + 1) * lanes)
            rate = log_sigmoid(d[way, :, cols].astype(jnp.float32)) / TAU
            high = rate.astype(jnp.bfloat16)
            rest = rate - high.astype(jnp.float32)
            mid = rest.astype(jnp.bfloat16)
            low = (rest - mid.astype(jnp.float32)).astype(jnp.bfloat16)
            cum[u] = contract(tri, high, NN) + contract(tri, mid, NN) + contract(tri, low, NN)
            state = jnp.zeros((VALUE_W, lanes), jnp.float32)
            reach = jnp.zeros((1, lanes), jnp.float32)
            lane = lax.broadcasted_iota(jnp.int32, (VALUE_W, lanes), 1) // key
            for n in range(blocks) if way == 0 else range(blocks - 1, -1, -1):
                rows = slice(n * BLOCK, (n + 1) * BLOCK)
                c = cum[u, rows, :]
                e = c[BLOCK - 1 : BLOCK] if way == 0 else c[0:1]
                queries = q[rows, cols].astype(jnp.float32) * key ** (-0.5)
                keys = k[rows, cols].astype(jnp.float32)
                qd[way, u, rows, :] = (queries * jnp.exp(c)).astype(jnp.bfloat16)
                kd[way, u, rows, :] = (keys * jnp.exp(-c)).astype(jnp.bfloat16)
                end = (keys * jnp.exp(e - c)).astype(jnp.bfloat16)
                term = None
                for h in range(per):
                    head = at * per + h
                    value = v[rows, head * VALUE_W : (head + 1) * VALUE_W]
                    new = contract(value, end, TN)
                    term = new if term is None else jnp.where(lane == h, new, term)
                added[way, u, n] = term
                fade = jnp.exp(e)
                ends[way, u, n : n + 1, :] = fade
                state = state * fade + term
                reach = reach + e
            sent[way, u * PACK : u * PACK + VALUE_W, :] = state.astype(jnp.bfloat16)
            if paired:
                row = way * count + u
                fade_own[row : row + 1, :] = jnp.exp(reach)
            else:
                sent[way, u * PACK + VALUE_W : (u + 1) * PACK, :] = jnp.broadcast_to(
                    jnp.exp(reach), (16, lanes)
                ).astype(jnp.bfloat16)

        if paired:
            for off in (1, 2, 3, 0):
                place_copy(u, off).start()
        else:

            @pl.loop(1, n_sp)
            def _(off):
                state_copy(u, off).start()

    if paired:

        @pl.loop(1, n_sp)
        def _(off):
            fade_copy(off).start()

    sent_states()
    t_blk = lax.broadcasted_iota(jnp.int32, (BLOCK, BLOCK), 0)
    s_blk = lax.broadcasted_iota(jnp.int32, (BLOCK, BLOCK), 1)
    first = 0
    for u, (q, k, v, g, d, norm, key, per, at) in enumerate(units):
        lane = lax.broadcasted_iota(jnp.int32, (BLOCK, lanes), 1) // key
        for h in range(per):
            head = at * per + h
            for n in range(blocks):
                rows = slice(n * BLOCK, (n + 1) * BLOCK)
                scores = None
                for way in range(2):
                    queries = qd[way, u, rows, :]
                    if per > 1:
                        queries = jnp.where(lane == h, queries, jnp.zeros_like(queries))
                    one = contract(queries, kd[way, u, rows, :], NT)
                    one = jnp.where((s_blk <= t_blk) if way == 0 else (s_blk >= t_blk), one, 0.0)
                    scores = one if scores is None else scores + one
                value = v[rows, head * VALUE_W : (head + 1) * VALUE_W]
                total[first + h, rows, :] = contract(scores.astype(jnp.bfloat16), value, NN)
        first += per

    carried[...] = jnp.zeros_like(carried)

    def fold(way, who):
        off = lax.rem(sp - who + n_sp, n_sp)
        for u in range(count):
            fade = got[off, u * PACK + VALUE_W : (u + 1) * PACK, :][0:1]
            state = got[off, u * PACK : u * PACK + VALUE_W, :]
            carried[way, u] = carried[way, u] * fade.astype(jnp.float32) + state.astype(jnp.float32)

    def fade_of(who, way, u):
        row = way * count + u
        return fade_all[lax.rem(sp - who + n_sp, n_sp), row : row + 1, :]

    def fold_place(way, u, z):
        off = lax.rem(place - z + GROUPS, GROUPS)
        fades = [fade_of(2 * z + y, way, u) for y in range(2)]
        state = got[off, u * PACK : u * PACK + VALUE_W, :].astype(jnp.float32)
        later = jnp.where(side == way, fades[1 - way], jnp.ones_like(fades[0]))
        carried[way, u] = carried[way, u] * (fades[0] * fades[1]) + state * later

    if paired:

        @pl.loop(1, n_sp)
        def _(off):
            fade_copy(off).wait()

        for u in range(count):
            for off in range(1, GROUPS):
                place_copy(u, off).wait()

            @pl.loop(0, place)
            def _(z):
                fold_place(0, u, z)

            @pl.loop(0, GROUPS - 1 - place)
            def _(back):
                fold_place(1, u, GROUPS - 1 - back)

            half_send[u] = carried[:, u].astype(jnp.bfloat16)
            half_copy(u).start()
        got_states()
        loaded()
        for u in range(count):
            place_copy(u, 0).wait()
            half_copy(u).wait()
            carried[:, u] = carried[:, u] + half_got[u].astype(jnp.float32)
            way = 1 - side
            off = 1 + way * (n_sp - 2)
            fade = fade_all[off, pl.ds(way * count + u, 1), :]
            state = got[0, u * PACK : u * PACK + VALUE_W, :].astype(jnp.float32)
            carried[way, u] = carried[way, u] * fade + state
    else:

        @pl.loop(1, n_sp)
        def _(off):
            for u in range(count):
                state_copy(u, off).wait()

        @pl.loop(0, sp)
        def _(who):
            fold(0, who)

        @pl.loop(0, n_sp - 1 - sp)
        def _(back):
            fold(1, n_sp - 1 - back)

    first = 0
    for u, (q, k, v, g, d, norm, key, per, at) in enumerate(units):
        lane = lax.broadcasted_iota(jnp.int32, (BLOCK, lanes), 1) // key
        for way in range(2):
            state = carried[way, u]
            for n in range(blocks) if way == 0 else range(blocks - 1, -1, -1):
                rows = slice(n * BLOCK, (n + 1) * BLOCK)
                low = state.astype(jnp.bfloat16)
                for h in range(per):
                    queries = qd[way, u, rows, :]
                    if per > 1:
                        queries = jnp.where(lane == h, queries, jnp.zeros_like(queries))
                    total[first + h, rows, :] += contract(queries, low, NT)
                state = state * ends[way, u, n : n + 1, :] + added[way, u, n]
        for h in range(per):
            head = at * per + h
            cols = slice(head * VALUE_W, (head + 1) * VALUE_W)
            x = total[first + h]
            y = x * lax.rsqrt(jnp.mean(x * x, axis=-1, keepdims=True) + EPS) * norm[...]
            gate = g[:, cols].astype(jnp.float32)
            y = y * (gate / (1.0 + jnp.exp(-gate)))
            mixed[:, (first + h) * VALUE_W : (first + h + 1) * VALUE_W] = y.astype(jnp.bfloat16)
        first += per

    rows_dev = res.shape[0]
    split = out1.shape[0]

    def project(mask):
        block = tp
        for bit in bits:
            if mask & bit:
                block = flip_bit(block, bit)
        rows = pl.ds(pl.multiple_of(block * rows_dev, 16), rows_dev)
        return contract(mixed[rows, :split], out1[...], NN) + contract(
            mixed[rows, split:], out2[...], NN
        )

    def part_copy(mask, bit):
        return remote(
            part_send.at[mask],
            part_got.at[mask],
            pt_send.at[mask],
            pt_recv.at[mask],
            (sp, flip_bit(tp, bit)),
        )

    low_bit = lambda m: m & -m
    order = sorted(range(1, n_tp), key=lambda m: (low_bit(m), -m))
    for mask in order:
        bit = low_bit(mask)
        value = project(mask)
        for earlier in bits:
            if earlier < bit:
                part_copy(mask | earlier, earlier).wait_recv()
                value = value + part_got[mask | earlier].astype(jnp.float32)
        part_send[mask] = value.astype(jnp.bfloat16)
        part_copy(mask, bit).start()
    sent_parts()
    value = project(0)
    for bit in bits:
        part_copy(bit, bit).wait_recv()
        value = value + part_got[bit].astype(jnp.float32)
    stream = (res[...].astype(jnp.float32) + value.astype(jnp.bfloat16).astype(jnp.float32)).astype(
        jnp.bfloat16
    )
    wide = stream.astype(jnp.float32)
    scale = lax.rsqrt(jnp.mean(wide * wide, axis=-1, keepdims=True) + EPS)
    normed = (wide * scale * gain[...]).astype(jnp.bfloat16)
    return stream, normed, [part_copy(mask, low_bit(mask)) for mask in order]


def mix_scratch(n_sp, n_tp, args, residual):
    q1, k1, v1, g1, d1, norm1, out1, q2, k2, v2, g2, d2, norm2, out2 = args
    length = q1.shape[0]
    blocks = length // BLOCK
    count = (q1.shape[1] + q2.shape[1]) // 128
    heads = (v1.shape[1] + v2.shape[1]) // VALUE_W
    rows, width = residual.shape
    packed = count * PACK
    bf, f32 = jnp.bfloat16, jnp.float32
    sem = pltpu.SemaphoreType.DMA
    return [
        pltpu.VMEM((count, length, 128), f32),
        pltpu.VMEM((2, count, length, 128), bf),
        pltpu.VMEM((2, count, length, 128), bf),
        pltpu.VMEM((2, count, blocks, VALUE_W, 128), f32),
        pltpu.VMEM((2, count, -(-blocks // 8) * 8, 128), f32),
        pltpu.VMEM((2, packed, 128), bf),
        pltpu.VMEM((n_sp, packed, 128), bf),
        pltpu.VMEM((2, count, VALUE_W, 128), f32),
        pltpu.VMEM((heads, length, VALUE_W), f32),
        pltpu.VMEM((length, heads * VALUE_W), bf),
        pltpu.VMEM((n_tp, rows, width), bf),
        pltpu.VMEM((n_tp, rows, width), bf),
        pltpu.VMEM((-(-2 * count // 8) * 8, 128), f32),
        pltpu.VMEM((n_sp, -(-2 * count // 8) * 8, 128), f32),
        pltpu.VMEM((count, 2, VALUE_W, 128), bf),
        pltpu.VMEM((count, 2, VALUE_W, 128), bf),
        sem((n_sp * count,)),
        sem((n_sp * count,)),
        sem((n_tp,)),
        sem((n_tp,)),
        sem((n_sp,)),
        sem((n_sp,)),
        sem((count,)),
        sem((count,)),
    ]


def mix_operands(args, residual, norm_gain):
    q1, k1, v1, g1, d1, norm1, out1, q2, k2, v2, g2, d2, norm2, out2 = args
    return (
        q1, k1, v1, g1, d1, q2, k2, v2, g2, d2,
        norm1[None], norm2[None], out1, out2, residual, norm_gain[None],
    )


def mixer_kernel(n_sp, n_tp, *refs):
    operands, (stream_ref, normed_ref), scratch = refs[:16], refs[16:18], refs[18:]
    ready = lambda go: [] if go is None else None
    stream, normed, pending = mix(
        n_sp, n_tp, operands, scratch, ready, nothing, nothing, nothing, nothing
    )
    stream_ref[...] = stream
    normed_ref[...] = normed
    for one in pending:
        one.wait_send()


def mixer(n_sp, n_tp, args, residual, norm_gain):
    rows, width = residual.shape
    vmem = pl.BlockSpec(memory_space=pltpu.VMEM)
    return pl.pallas_call(
        functools.partial(mixer_kernel, n_sp, n_tp),
        out_shape=(jax.ShapeDtypeStruct((rows, width), jnp.bfloat16),) * 2,
        in_specs=[vmem] * 16,
        out_specs=(vmem, vmem),
        scratch_shapes=mix_scratch(n_sp, n_tp, args, residual),
        compiler_params=pltpu.CompilerParams(
            collective_id=0, has_side_effects=True, vmem_limit_bytes=60 * 2**20
        ),
    )(*mix_operands(args, residual, norm_gain))


ORDER = ((0, 1, 2, 3), (1, 3, 2, 0))
SEND = ((0, 2, 1, 3), (1, 0, 3, 2))


def mirror(place):
    turned, last = place // (GROUPS // 2), GROUPS - 1
    return turned, place + turned * (last - 2 * place)


def place_at(place, rank, table):
    turned, inner = mirror(place)
    end, mid = table[0][rank], table[1][rank]
    spot = end + inner * (mid - end)
    return spot + turned * (GROUPS - 1 - 2 * spot)


def rank_in(place, other, table):
    turned, inner = mirror(place)
    spot = other + turned * (GROUPS - 1 - 2 * other)
    end, mid = (
        sum(jnp.where(spot == row[rank], rank, 0) for rank in range(GROUPS)) for row in table
    )
    return end + inner * (mid - end)


KINDS = 5
COPIES = 10 * GROUPS + 4 * GROUPS + 8


def layer_kernel(n_sp, n_tp, stride, over, extra, n_scratch, *refs):
    given = refs[:16]
    ids, group_share, pair_share, w_gate, w_up, w_down, out_ref = refs[16:23]
    scratch = refs[23 : 23 + n_scratch]
    operands = refs[23 + n_scratch : 39 + n_scratch]
    (
        v_gate, v_up, wd, spread, meta_send, meta_got, wslot, z_send, z_extra, data, hid, hgot,
        acc, part, pgot, outs, back_got, kept, w_sem, o_sem, s_sem, r_sem, zs_sem, zr_sem,
    ) = refs[39 + n_scratch :]
    bf, f32 = jnp.bfloat16, jnp.float32
    sp, tp = lax.axis_index("sp"), lax.axis_index("tp")
    span = stride + extra
    length = GROUPS * stride + extra
    wire = -(-GROUPS * over // 8) * 8
    width = data.shape[2]
    units = hid.shape[2]
    place, side = sp // 2, lax.rem(sp, 2)
    core, across, along = (sp, flip_bit(tp, 1)), (sp, flip_bit(tp, 2)), (flip_bit(sp, 1), tp)
    corner = (flip_bit(sp, 1), flip_bit(tp, 2))
    cut = width // 256 * 128
    left, right = slice(0, cut), slice(cut, width)
    far, home = [], []
    for i in range(1, GROUPS):
        z = place_at(place, i, SEND)
        far.append((i, rank_in(z, place, ORDER), (z * 2 + side, tp)))
        z = place_at(place, i, ORDER)
        home.append((i, rank_in(z, place, SEND), (z * 2 + side, tp)))
    numbers = iter(range(COPIES))
    started = []

    def copy(source, target, device):
        number = next(numbers)
        return remote(source, target, s_sem.at[number], r_sem.at[number], device)

    def go(one):
        one.start()
        started.append(one)
        return one

    def z_copy(kind, i, rank, source, target, device):
        return remote(
            source,
            target,
            zs_sem.at[kind * GROUPS + i],
            zr_sem.at[kind * GROUPS + rank],
            device,
        )

    loads = [
        pltpu.make_async_copy(source, target, w_sem.at[i])
        for i, (source, target) in enumerate(
            ((w_gate, v_gate), (w_up, v_up), (w_down, wd.at[0]))
        )
    ]
    late = (3, 8, 10, 11, 12, 13, 14, 15)
    moves = [
        pltpu.make_async_copy(given[i], operands[i], o_sem.at[i]) for i in range(len(operands))
    ]
    quarter = units // 4
    down_y = [
        copy(w_down.at[rows], wd.at[1, rows], along)
        for rows in (
            slice(0, quarter), slice(quarter, 3 * quarter), slice(3 * quarter, units)
        )
    ]
    down_x = copy(w_down, wd.at[2], across)
    upper, middle = slice(0, quarter), slice(quarter, 2 * quarter)
    lower = slice(2 * quarter, units)
    down_yx = [copy(wd.at[1, rows], wd.at[3, rows], across) for rows in (upper, middle)]
    down_xy = copy(wd.at[2, lower], wd.at[3, lower], along)
    metas = [
        z_copy(4, i, rank, meta_send.at[slice(i * span, (i + 1) * span)], meta_got.at[rank], to)
        for i, rank, to in far
    ]
    meta_core = copy(wslot.at[0], wslot.at[1], core)

    def block(index):
        return slice(index * span, (index + 1) * span)

    def chunk(o):
        return slice(o * stride, (o + 1) * stride if o < GROUPS - 1 else length)

    def moved(o):
        return slice(o * stride, (o + 1) * stride if o < GROUPS - 1 else GROUPS * stride + wire)

    def routing():
        rows, tokens = spread.shape[1], ids.shape[1]
        first, share = ids[0:1, :], group_share[...]
        kind = lax.broadcasted_iota(jnp.int32, (8, 1), 0)
        member = ((first >= 2 * kind) & (first < 2 * kind + 2)).astype(f32)
        from_at = lax.broadcasted_iota(jnp.int32, (tokens, tokens), 0)
        to_at = lax.broadcasted_iota(jnp.int32, (tokens, tokens), 1)
        before = jnp.where((from_at < to_at) & (from_at // rows == to_at // rows), 1.0, 0.0)
        counts = contract(member.astype(bf), before.astype(bf), NN)
        nth = jnp.sum(member * counts, axis=0, keepdims=True)
        named = lax.rem(kind, GROUPS)
        base = (rank_in(place, named, SEND) * span).astype(f32)
        shift = (rank_in(named, place, ORDER) * over).astype(f32)
        seat = base + jnp.where(nth < stride, nth, nth + shift)
        seat = jnp.sum(member * seat, axis=0, keepdims=True)
        pair = pair_share[0:1, :] + pair_share[1:2, :]
        w_first = share * pair_share[0:1, :] / pair
        w_second = share * pair_share[1:2, :] / pair
        even = lax.rem(first, 2) == 0
        table = jnp.zeros((8, tokens), f32)
        table = jnp.where(kind == 0, seat, table)
        for s in range(2):
            w = jnp.where(even, w_first, w_second) if s == 0 else jnp.where(even, w_second, w_first)
            high = w.astype(bf).astype(f32)
            table = jnp.where(kind == 1 + s, high, table)
            table = jnp.where(kind == 3 + s, w - high, table)
        at = lax.broadcasted_iota(jnp.int32, (tokens, rows), 0)
        own_at = lax.broadcasted_iota(jnp.int32, (tokens, rows), 1) + tp * rows
        select = jnp.where(at == own_at, 1.0, 0.0).astype(bf)
        table = contract(table.astype(bf), select, NN)
        seats = lax.broadcasted_iota(jnp.int32, (GROUPS * span, rows), 0)
        spread[...] = jnp.where(seats == table[0:1].astype(jnp.int32), 1.0, 0.0).astype(bf)
        line = lax.broadcasted_iota(jnp.int32, (128, 1), 0)
        lines = jnp.zeros((128, rows), f32)
        for row, spot in ((1, 0), (2, 1), (3, 64), (4, 65)):
            lines = jnp.where(line == spot, table[row : row + 1], lines)
        meta_send[...] = contract(spread[...], lines.astype(bf), NT).astype(bf)

    def ready(begin):
        if begin is None:
            return [corner]
        go(down_x)
        go(down_y[0])
        for load in loads:
            load.start()
        for i, move in enumerate(moves):
            if i not in late:
                move.wait()

    def sent_states():
        go(down_y[1])
        routing()
        for one in metas:
            go(one)
        rest = slice(GROUPS * stride + wire, length)
        if wire < extra:
            data[:, rest, :] = jnp.zeros((8, extra - wire, width), bf)
            hgot[:, :, rest, :] = jnp.zeros((3, 2, extra - wire, units), bf)
            pgot[rest, :] = jnp.zeros((extra - wire, width), bf)
            for i in range(GROUPS):
                spare = slice(i * span + stride + wire, (i + 1) * span)
                back_got[spare, :] = jnp.zeros((extra - wire, width), bf)
    def loaded():
        for i in late:
            moves[i].wait()

    def sent_parts():
        down_y[1].wait_recv()
        go(down_yx[1])
        down_x.wait_recv()
        go(down_xy)

    def meta_wait(o):
        z_copy(4, 0, o, meta_send.at[block(o)], meta_got.at[o], core).wait_recv()

    def got_states():
        own = meta_send[block(0)]
        wslot[0, 0:stride] = own[:stride]
        more = own[stride:].astype(f32)
        for o in range(1, GROUPS):
            meta_wait(o)
            wslot[0, o * stride : (o + 1) * stride] = meta_got[o, :stride]
            more = more + meta_got[o, stride:].astype(f32)
        wslot[0, GROUPS * stride :] = more.astype(bf)
        go(meta_core)
        down_y[0].wait_recv()
        go(down_yx[0])
        go(down_y[2])

    for i in sorted(range(len(moves)), key=lambda i: i in late):
        moves[i].start()
    stream, normed, pending = mix(
        n_sp, n_tp, operands, scratch, ready, sent_states, loaded, got_states, sent_parts
    )
    kept[...] = stream

    for i, rank, to in far:
        z_send[block(i)] = contract(spread[block(i), :], normed, NN).astype(bf)
        go(
            z_copy(
                0, i, rank,
                z_send.at[slice(i * span, i * span + stride)],
                data.at[0, pl.ds(pl.multiple_of(rank * stride, 16), stride)],
                to,
            )
        )
        go(
            z_copy(
                1, i, rank,
                z_send.at[slice(i * span + stride, i * span + stride + wire)],
                z_extra.at[rank],
                to,
            )
        )
    own = contract(spread[block(0), :], normed, NN).astype(bf)
    data[0, chunk(0), :] = own[:stride]
    z_extra[0] = own[stride : stride + wire]

    flows = []
    for o in range(GROUPS):
        ch = moved(o)
        flows.append(
            dict(
                a_y=copy(data.at[0, ch, left], data.at[2, ch, left], along),
                b_x=copy(data.at[0, ch, right], data.at[4, ch, right], across),
                a_x=copy(data.at[0, ch, left], data.at[4, ch, left], across),
                b_y=copy(data.at[0, ch, right], data.at[2, ch, right], along),
                c_0=copy(data.at[0, ch], data.at[1, ch], core),
                a_d=copy(data.at[2, ch, left], data.at[6, ch, left], across),
                b_d=copy(data.at[4, ch, right], data.at[6, ch, right], along),
                c_y=copy(data.at[2, ch], data.at[3, ch], core),
                c_x=copy(data.at[4, ch], data.at[5, ch], core),
                c_d=copy(data.at[6, ch], data.at[7, ch], core),
                h_y=copy(hid.at[slice(2, 4), ch], hgot.at[0, :, ch], along),
                h_x=copy(hid.at[slice(4, 6), ch], hgot.at[1, :, ch], across),
                h_d=copy(hid.at[slice(6, 8), ch], hgot.at[2, :, ch], corner),
                p_c=copy(part.at[ch], pgot.at[ch], core),
            )
        )

    def arrive(kind, o, target):
        z_copy(kind, 0, o, target, target, core).wait_recv()

    def stage(o):
        flow = flows[o]
        if o:
            arrive(0, o, data.at[0, slice(o * stride, (o + 1) * stride)])
        if o == GROUPS - 1:
            more = z_extra[0].astype(f32)
            for k in range(1, GROUPS):
                arrive(1, k, z_extra.at[k])
                more = more + z_extra[k].astype(f32)
            data[0, GROUPS * stride : GROUPS * stride + wire, :] = more.astype(bf)
        for name in ("a_y", "b_x", "a_x", "b_y", "c_0"):
            go(flow[name])

    def forward(o):
        flow = flows[o]
        flow["a_y"].wait_recv()
        go(flow["a_d"])
        flow["b_x"].wait_recv()
        go(flow["b_d"])
        flow["b_y"].wait_recv()
        go(flow["c_y"])
        flow["a_x"].wait_recv()
        go(flow["c_x"])

    def finish(o):
        flow = flows[o]
        flow["a_d"].wait_recv()
        flow["b_d"].wait_recv()
        go(flow["c_d"])

    def compute(o, part_at):
        flow, ch = flows[o], chunk(o)
        for name in (("c_0", "c_y"), ("c_x", "c_d"))[part_at]:
            flow[name].wait_recv()
        n = ch.stop - ch.start

        @pl.loop(part_at, part_at + 1)
        def _(m):
            some = pl.ds(m * 4, 4)
            x = data[some, ch, :].reshape(4 * n, width)
            gate = contract(x, v_gate[...], NN)
            up = contract(x, v_up[...], NN)
            hidden = (gate / (1.0 + jnp.exp(-gate)) * up).astype(bf)
            hid[some, ch, :] = hidden.reshape(4, n, units)

        for name in (("h_y",), ("h_d", "h_x"))[part_at]:
            go(flow[name])

    lane = lax.broadcasted_iota(jnp.int32, (1, 128), 1)

    def down(o):
        flow, ch = flows[o], chunk(o)
        n = ch.stop - ch.start
        w = wslot[:, ch, :].reshape(2 * n, 128).astype(f32)
        pick = lambda s: jnp.sum(
            jnp.where((lane == s) | (lane == s + 64), w, 0.0), axis=1, keepdims=True
        )
        mine, other = pick(side), pick(1 - side)
        for name in ("h_y", "h_x", "h_d"):
            flow[name].wait_recv()
        tile = 512

        @pl.loop(0, width // tile)
        def _(j):
            cols = pl.ds(pl.multiple_of(j * tile, tile), tile)
            rows = lambda value: value.reshape(2 * n, units)
            a = contract(rows(hid[0:2, ch, :]), wd[0, :, cols], NN) + contract(
                rows(hgot[1, :, ch, :]), wd[2, :, cols], NN
            )
            b = contract(rows(hgot[0, :, ch, :]), wd[1, :, cols], NN) + contract(
                rows(hgot[2, :, ch, :]), wd[3, :, cols], NN
            )
            value = a * mine + b * other
            acc[ch, cols] = value[:n]
            part[ch, cols] = value[n:].astype(bf)

        go(flow["p_c"])

    def give(o):
        flow, ch = flows[o], chunk(o)
        flow["p_c"].wait_recv()
        outs[ch, :] = (acc[ch, :] + pgot[ch, :].astype(f32)).astype(bf)
        rows = slice(o * stride, (o + 1) * stride)
        if o == 0:
            back_got[0:stride] = outs[rows, :]
        else:
            i, rank, to = home[o - 1]
            go(
                z_copy(
                    2, i, rank,
                    outs.at[rows],
                    back_got.at[pl.ds(pl.multiple_of(rank * span, 16), stride)],
                    to,
                )
            )
        if o == GROUPS - 1:
            rows = slice(GROUPS * stride, GROUPS * stride + wire)
            back_got[stride : stride + wire] = outs[rows, :]
            for i, rank, to in home:
                go(
                    z_copy(
                        3, i, rank,
                        outs.at[rows],
                        back_got.at[pl.ds(pl.multiple_of(rank * span + stride, 16), wire)],
                        to,
                    )
                )

    stage(0)
    forward(0)
    for load in loads:
        load.wait()
    compute(0, 0)
    finish(0)
    compute(0, 1)
    stage(1)
    forward(1)
    stage(2)
    compute(1, 0)
    finish(1)
    compute(1, 1)
    forward(2)
    stage(3)
    meta_core.wait_recv()
    for one in (down_y[2], *down_yx, down_xy):
        one.wait_recv()
    down(0)
    down(1)
    compute(2, 0)
    finish(2)
    compute(2, 1)
    give(1)
    forward(3)
    down(2)
    compute(3, 0)
    finish(3)
    compute(3, 1)
    give(2)
    give(0)
    down(3)
    give(3)
    for i in range(1, GROUPS):
        arrive(2, i, back_got.at[slice(i * span, i * span + stride)])
        arrive(3, i, back_got.at[slice(i * span + stride, i * span + stride + wire)])
    picked = contract(spread[...], back_got[...], TN)
    out_ref[...] = (kept[...].astype(f32) + picked).astype(bf)
    for one in pending + started:
        one.wait_send()


def whole_layer(n_sp, n_tp, args, residual, norm_gain, routing, capacity, w_gate, w_up, w_down):
    rows, width = residual.shape
    units = w_gate.shape[1]
    stride = capacity // 16 * 16
    over = capacity - stride
    extra = max(16, -(-GROUPS * over // 16) * 16)
    span, length = stride + extra, GROUPS * stride + extra
    bf, f32 = jnp.bfloat16, jnp.float32
    vmem = pl.BlockSpec(memory_space=pltpu.VMEM)
    hbm = pl.BlockSpec(memory_space=pl.ANY)
    sem = pltpu.SemaphoreType.DMA
    mine = mix_scratch(n_sp, n_tp, args, residual)
    given = mix_operands(args, residual, norm_gain)
    return pl.pallas_call(
        functools.partial(layer_kernel, n_sp, n_tp, stride, over, extra, len(mine)),
        out_shape=jax.ShapeDtypeStruct((rows, width), bf),
        in_specs=[hbm] * 16 + [vmem] * 3 + [hbm] * 3,
        out_specs=vmem,
        scratch_shapes=mine
        + [pltpu.VMEM(one.shape, one.dtype) for one in given]
        + [
            pltpu.VMEM(w_gate.shape, bf),
            pltpu.VMEM(w_up.shape, bf),
            pltpu.VMEM((4, units, width), bf),
            pltpu.VMEM((GROUPS * span, rows), bf),
            pltpu.VMEM((GROUPS * span, 128), bf),
            pltpu.VMEM((GROUPS, span, 128), bf),
            pltpu.VMEM((2, length, 128), bf),
            pltpu.VMEM((GROUPS * span, width), bf),
            pltpu.VMEM((GROUPS, -(-GROUPS * over // 8) * 8, width), bf),
            pltpu.VMEM((8, length, width), bf),
            pltpu.VMEM((8, length, units), bf),
            pltpu.VMEM((3, 2, length, units), bf),
            pltpu.VMEM((length, width), f32),
            pltpu.VMEM((length, width), bf),
            pltpu.VMEM((length, width), bf),
            pltpu.VMEM((length, width), bf),
            pltpu.VMEM((GROUPS * span, width), bf),
            pltpu.VMEM((rows, width), bf),
            sem((3,)),
            sem((16,)),
            sem((COPIES,)),
            sem((COPIES,)),
            sem((KINDS * GROUPS,)),
            sem((KINDS * GROUPS,)),
        ],
        compiler_params=pltpu.CompilerParams(
            collective_id=1, has_side_effects=True, vmem_limit_bytes=63 * 2**20
        ),
    )(*given, *routing, w_gate, w_up, w_down)


def slot_table(routes, capacity, experts):
    flat = routes.reshape(-1)
    count = flat.shape[0]
    onehot = (flat[:, None] == jnp.arange(experts, dtype=jnp.int32)[None, :]).astype(jnp.int32)
    place = jnp.sum((jnp.cumsum(onehot, axis=0) - onehot) * onehot, axis=1)
    table = (
        jnp.full((experts, capacity), count, jnp.int32)
        .at[flat, place]
        .set(jnp.arange(count, dtype=jnp.int32))
    )
    return (table, place)

def body(
    residual,
    query_one,
    key_one,
    value_one,
    gate_one,
    decay_one,
    norm_one,
    output_one,
    query_two,
    key_two,
    value_two,
    gate_two,
    decay_two,
    norm_two,
    output_two,
    norm_gain,
    expert_ids,
    group_weight,
    pair_weight,
    expert_gate,
    expert_up,
    expert_down,
):
    n_sp, n_tp = lax.axis_size("sp"), lax.axis_size("tp")
    mixing = (
        query_one, key_one, value_one, gate_one, decay_one, norm_one, output_one,
        query_two, key_two, value_two, gate_two, decay_two, norm_two, output_two,
    )
    rows_dev = residual.shape[0]
    rank = lax.axis_index("tp")
    experts = n_sp
    capacity = max(2, 2 * rows_dev // (experts - GROUPS) + 1)
    if experts == 2 * GROUPS and n_tp == 4:
        return whole_layer(
            n_sp,
            n_tp,
            mixing,
            residual,
            norm_gain,
            (expert_ids.T, group_weight[None], pair_weight.T),
            capacity,
            expert_gate[0],
            expert_up[0],
            expert_down[0],
        )
    own_routes = lax.dynamic_slice_in_dim(expert_ids, rank * rows_dev, rows_dev, 0)
    own_group = lax.dynamic_slice_in_dim(group_weight, rank * rows_dev, rows_dev, 0)
    own_pair = lax.dynamic_slice_in_dim(pair_weight, rank * rows_dev, rows_dev, 0)
    weights = own_group[:, None] * own_pair / jnp.sum(own_pair, axis=1, keepdims=True)
    stream, normed_rows = mixer(n_sp, n_tp, mixing, residual, norm_gain)
    blank = jnp.zeros((1, D), jnp.bfloat16)
    table, own_place = slot_table(own_routes, capacity, experts)
    index = jnp.where(table == 2 * rows_dev, rows_dev, table // 2)
    send = jnp.concatenate([normed_rows, blank], axis=0)[index][None]
    received = lax.all_to_all(send, "sp", split_axis=1, concat_axis=1, tiled=True)
    received = lax.all_gather(received, "tp", axis=0, tiled=True)
    flat = received.reshape(-1, received.shape[-1])
    gate_part = jnp.dot(flat, expert_gate[0], preferred_element_type=jnp.float32)
    up_part = jnp.dot(flat, expert_up[0], preferred_element_type=jnp.float32)
    hidden = (jax.nn.silu(gate_part) * up_part).astype(jnp.bfloat16)
    share_sum = lax.psum_scatter(
        jnp.dot(hidden, expert_down[0], preferred_element_type=jnp.float32)
        .reshape(received.shape)
        .astype(jnp.bfloat16),
        "tp",
        scatter_dimension=0,
        tiled=True,
    )
    returned = lax.all_to_all(share_sum, "sp", split_axis=1, concat_axis=1, tiled=True)
    slot_index = own_routes.reshape(-1) * capacity + own_place
    picked = returned.reshape(-1, D)[slot_index].astype(jnp.float32).reshape(rows_dev, 2, D)
    layer = stream.astype(jnp.float32) + jnp.sum(weights[:, :, None] * picked, axis=1)
    return layer.astype(jnp.bfloat16)

def solution(mesh):
    placed = (
        P(("sp", "tp"), None),
        P("sp", "tp"),
        P("sp", "tp"),
        P("sp", "tp"),
        P("sp", "tp"),
        P(None, "sp", "tp"),
        P(),
        P("tp", None),
        P("sp", "tp"),
        P("sp", "tp"),
        P("sp", "tp"),
        P("sp", "tp"),
        P(None, "sp", "tp"),
        P(),
        P("tp", None),
        P(),
        P("sp", None),
        P("sp"),
        P("sp", None),
        P("sp", None, "tp"),
        P("sp", None, "tp"),
        P("sp", "tp", None),
    )
    return jax.shard_map(
        body, mesh=mesh, in_specs=placed, out_specs=P(("sp", "tp"), None), check_vma=False
    )
```
